32 devices in a mesh: grp: 2 (over y), sp: 8 (over z, core), tp: 2 (over x).
Axes of the slice: x: 2, y: 2, z: 4, core: 2. Of those that a mesh axis runs over, the one named last changes fastest.
Arguments:
- layer_input: bfloat16 [3072, 2048], P(('grp', 'sp', 'tp')), parts along dimension 0, may hold values from -6 to 6
- latent: bfloat16 [3072, 512], P(('grp', 'sp')), parts along dimension 0, may hold values from -6 to 6
- rope_key: bfloat16 [3072, 64], P(('grp', 'sp')), parts along dimension 0, may hold values from -4 to 4
- query_wide: bfloat16 [3072, 1536], P(('grp', 'sp'), 'tp'), parts along dimension 0, may hold values from -18 to 18
- query_narrow: bfloat16 [3072, 1024], P(('grp', 'sp'), 'tp'), parts along dimension 0, may hold values from -18 to 18
- key_up_wide: bfloat16 [512, 1024], P(None, 'tp'), may hold values from -0.25 to 0.25
- value_up_wide: bfloat16 [512, 1024], P(None, 'tp'), may hold values from -0.25 to 0.25
- key_up_narrow: bfloat16 [512, 512], P(None, 'tp'), may hold values from -0.25 to 0.25
- value_up_narrow: bfloat16 [512, 512], P(None, 'tp'), may hold values from -0.25 to 0.25
- out_wide: bfloat16 [1024, 2048], P('tp'), may hold values from -1.1953125 to 1.1953125
- out_narrow: bfloat16 [512, 2048], P('tp'), may hold values from -1.1953125 to 1.1953125
- norm_gain: float32 [2048], replicated, may hold values from 0.1 to 1.9
- gate_weight: bfloat16 [2048, 5632], P('sp', 'tp'), may hold values from -0.125 to 0.125
- value_weight: bfloat16 [2048, 5632], P('sp', 'tp'), may hold values from -0.125 to 0.125
- conv_weight: float32 [3, 5632], P(None, 'tp'), may hold values from -2.5 to 2.5
- down_weight: bfloat16 [5632, 2048], P('tp', 'sp'), may hold values from -0.078125 to 0.078125
Outputs:
- layer_output: bfloat16 [3072, 2048], P(('grp', 'sp', 'tp')), parts along dimension 0
The draws below stay inside these ranges and needn't reach their ends.
There are 2 independent parts, one for each index of `grp`. The reference program is written for one: setup_inputs(seed, part) draws one part's arguments, and reference() takes and returns one part's arrays. A program takes and returns all parts, laid end to end along the dimension named above; an argument that names none is the same for every part. Nothing has to cross between parts.
All inputs are finite; a program needn't handle non-finite values.
Results may differ from the reference program's by a relative error of at most 0.015.
Values may be sent and summed in bfloat16 or wider, within the bound.
A program may use at most 128 MiB of HBM per device.

```python
import math
import jax
import jax.numpy as jnp
from jax import lax

D = 2048
LATENT = 512
ROT = 64
NOPE_W = 128
VAL_W = 128
NOPE_N = 64
VAL_N = 64
HEADS_W = 8
HEADS_N = 8
FF = 5632
CONV = 3
TOK_DEV = 192
TOKENS = 1536
N_TP = 2


def planted_rows(key):
    positions = jnp.arange(TOKENS, dtype=jnp.int32)
    planted = jax.random.randint(jax.random.fold_in(key, 101), (TOKENS,), 0, 48) == 0
    offsets = jax.random.randint(jax.random.fold_in(key, 103), (TOKENS,), TOK_DEV, TOKENS - TOK_DEV + 1)
    target = (positions + offsets) % TOKENS
    rotary = jnp.clip(jax.random.normal(jax.random.fold_in(key, 102), (TOKENS, ROT), jnp.float32), -4.0, 4.0)
    return (planted, target, rotary)


def planted_query(key, head_count, nope_width, salt_value):
    planted, target, rotary = planted_rows(key)
    own_key = jax.random.fold_in(key, salt_value)
    drawn = jnp.clip(2.0 * jax.random.normal(own_key, (TOKENS, head_count, nope_width + ROT), jnp.float32), -12.0, 12.0)
    return drawn.reshape(TOKENS, head_count * (nope_width + ROT))


def draw_rope_key(key, part):
    return planted_rows(key)[2].astype(jnp.bfloat16)


def draw_query_wide(key, part):
    return planted_query(key, HEADS_W, NOPE_W, 201).astype(jnp.bfloat16)


def draw_query_narrow(key, part):
    return planted_query(key, HEADS_N, NOPE_N, 202).astype(jnp.bfloat16)


def block_scale(key, dims, shards, least, top_value):
    def one(axis_at, blocks):
        steps = jax.random.uniform(jax.random.fold_in(jax.random.fold_in(key, 6), axis_at), (blocks,), jnp.float32, least / len(shards), top_value / len(shards))
        return jnp.repeat(jnp.exp(steps), dims[axis_at] // blocks).reshape((-1,) + (1,) * (len(dims) - axis_at - 1))

    loudness = one(*shards[0])
    for cut in shards[1:]:
        loudness = loudness * one(*cut)
    return loudness


def centred(stream_key, extent, deviation, bound, cuts=(), kind=jnp.bfloat16):
    values = deviation * jax.random.normal(stream_key, extent, jnp.float32)
    if cuts:
        values = values * block_scale(stream_key, extent, cuts, -0.22, 0.18)
    return jnp.clip(values, -bound, bound).astype(kind)


def setup_inputs(seed: int = 0, part: int = 0) -> dict:
    key_of = jax.random.split(jax.random.key(seed), 17)
    own_keys = jax.random.split(jax.random.fold_in(key_of[16], part), 17)
    return {
        "layer_input": centred(own_keys[0], (TOKENS, D), 1.0, 6.0, ((0, 16),)),
        "latent": centred(own_keys[1], (TOKENS, LATENT), 1.0, 6.0, ((0, 8),)),
        "rope_key": draw_rope_key(jax.random.fold_in(jax.random.fold_in(key_of[16], part), 71), part),
        "query_wide": draw_query_wide(jax.random.fold_in(jax.random.fold_in(key_of[16], part), 71), part),
        "query_narrow": draw_query_narrow(jax.random.fold_in(jax.random.fold_in(key_of[16], part), 71), part),
        "key_up_wide": centred(key_of[5], (LATENT, HEADS_W * NOPE_W), LATENT ** -0.5, 0.25, ((1, 2),)),
        "value_up_wide": centred(key_of[6], (LATENT, HEADS_W * VAL_W), LATENT ** -0.5, 0.25, ((1, 2),)),
        "key_up_narrow": centred(key_of[7], (LATENT, HEADS_N * NOPE_N), LATENT ** -0.5, 0.25, ((1, 2),)),
        "value_up_narrow": centred(key_of[8], (LATENT, HEADS_N * VAL_N), LATENT ** -0.5, 0.25, ((1, 2),)),
        "out_wide": centred(key_of[9], (HEADS_W * VAL_W, D), 0.2, 1.1953125, ((0, 2),)),
        "out_narrow": centred(key_of[10], (HEADS_N * VAL_N, D), 0.2, 1.1953125, ((0, 2),)),
        "norm_gain": jnp.clip(1.0 + 0.18 * jax.random.normal(key_of[11], (D,), jnp.float32), 0.1, 1.9),
        "gate_weight": centred(key_of[12], (D, FF), D ** -0.5, 0.125, ((0, 8), (1, 2))),
        "value_weight": centred(key_of[13], (D, FF), D ** -0.5, 0.125, ((0, 8), (1, 2))),
        "conv_weight": centred(key_of[14], (CONV, FF), 0.6, 2.5, ((1, 2),), jnp.float32),
        "down_weight": centred(key_of[15], (FF, D), FF ** -0.5, 0.078125, ((0, 2), (1, 8))),
    }


rope_base = 10000.0
norm_eps = 1e-06

def rope_tables(row_total, span_width):
    places = jnp.arange(row_total, dtype=jnp.int32).astype(jnp.float32)
    frequency = jnp.power(rope_base, -jnp.arange(0, span_width, 2, dtype=jnp.int32).astype(jnp.float32) / span_width)
    angles = places[:, None] * frequency[None, :]
    angles = jnp.concatenate([angles, angles], axis=-1)
    return (jnp.cos(angles), jnp.sin(angles))

def spin_rows(entries, cosine, sine_table):
    entries = entries.astype(jnp.float32)
    lead_half, tail_half = jnp.split(entries, 2, axis=-1)
    return entries * cosine + jnp.concatenate([-tail_half, lead_half], axis=-1) * sine_table

def group_attention(query, latent, turned_key, key_up, value_up, head_count, nope_width, value_width, cosine, sine_table):
    rot_width = turned_key.shape[1]
    shaped = query.reshape(TOKENS, head_count, nope_width + rot_width)
    nope_q = shaped[:, :, :nope_width]
    rope_q = spin_rows(shaped[:, :, nope_width:], cosine[:, None, :], sine_table[:, None, :]).astype(jnp.bfloat16)
    key_rows = jnp.dot(latent, key_up, preferred_element_type=jnp.float32).astype(jnp.bfloat16)
    key_rows = key_rows.reshape(TOKENS, head_count, nope_width).astype(jnp.float32)
    value_rows = jnp.dot(latent, value_up, preferred_element_type=jnp.float32).astype(jnp.bfloat16)
    value_rows = value_rows.reshape(TOKENS, head_count, value_width).astype(jnp.float32)
    key_turned = turned_key.astype(jnp.float32)
    score_scale = 1.0 / math.sqrt(nope_width + rot_width)

    def one_block(query_block):
        nope_block, rope_block = query_block
        scores = jnp.einsum('qhd,khd->qhk', nope_block.astype(jnp.float32), key_rows)
        scores = (scores + jnp.einsum('qhd,kd->qhk', rope_block.astype(jnp.float32), key_turned)) * score_scale
        weights = jnp.exp(scores - lax.optimization_barrier(jnp.max(scores, axis=-1, keepdims=True)))
        row_sum = lax.optimization_barrier(jnp.sum(weights, axis=-1))
        rounded = lax.optimization_barrier(weights.astype(jnp.bfloat16)).astype(jnp.float32)
        mixed = jnp.einsum('qhk,khd->qhd', rounded, value_rows)
        return (mixed / row_sum[:, :, None]).astype(jnp.bfloat16)
    blocks = TOKENS // TOK_DEV
    nope_blocks = nope_q.reshape(blocks, TOK_DEV, head_count, nope_width)
    rope_blocks = rope_q.reshape(blocks, TOK_DEV, head_count, rot_width)
    result = lax.map(one_block, (nope_blocks, rope_blocks))
    return result.reshape(TOKENS, head_count * value_width)

def reference(layer_input, latent, rope_key, query_wide, query_narrow, key_up_wide, value_up_wide, key_up_narrow, value_up_narrow, out_wide, out_narrow, norm_gain, gate_weight, value_weight, conv_weight, down_weight):
    cosine, sine_table = rope_tables(TOKENS, ROT)
    turned_key = spin_rows(rope_key, cosine, sine_table).astype(jnp.bfloat16)
    wide_att = group_attention(query_wide, latent, turned_key, key_up_wide, value_up_wide, HEADS_W, NOPE_W, VAL_W, cosine, sine_table)
    narrow_att = group_attention(query_narrow, latent, turned_key, key_up_narrow, value_up_narrow, HEADS_N, NOPE_N, VAL_N, cosine, sine_table)
    wide_share = HEADS_W * VAL_W // N_TP
    narrow_share = HEADS_N * VAL_N // N_TP
    head_part = jnp.einsum('tic,icd->itd', wide_att.reshape(TOKENS, N_TP, wide_share).astype(jnp.float32), out_wide.reshape(N_TP, wide_share, D).astype(jnp.float32))
    head_part = head_part + jnp.einsum('tic,icd->itd', narrow_att.reshape(TOKENS, N_TP, narrow_share).astype(jnp.float32), out_narrow.reshape(N_TP, narrow_share, D).astype(jnp.float32))
    head_part = lax.optimization_barrier(head_part.astype(jnp.bfloat16)).astype(jnp.float32)
    middle = (layer_input.astype(jnp.float32) + lax.optimization_barrier(jnp.sum(head_part, axis=0))).astype(jnp.bfloat16)
    middle_full = middle.astype(jnp.float32)
    normed = middle_full * lax.rsqrt(lax.optimization_barrier(jnp.mean(middle_full * middle_full, axis=-1, keepdims=True)) + norm_eps)
    normed = (normed * norm_gain).astype(jnp.bfloat16)
    gate_pre = jnp.dot(normed, gate_weight, preferred_element_type=jnp.float32).astype(jnp.bfloat16)
    value_pre = jnp.dot(normed, value_weight, preferred_element_type=jnp.float32)
    padded = jnp.pad(gate_pre, ((1, 1), (0, 0))).astype(jnp.float32)
    conv_gate = jnp.zeros((TOKENS, FF), jnp.float32)
    for kernel_tap in range(CONV):
        conv_gate = conv_gate + conv_weight[kernel_tap] * padded[kernel_tap:kernel_tap + TOKENS]
    hidden = (jax.nn.silu(conv_gate) * value_pre).astype(jnp.bfloat16)
    hidden_share = FF // N_TP
    channel_part = jnp.einsum('tic,icd->itd', hidden.reshape(TOKENS, N_TP, hidden_share).astype(jnp.float32), down_weight.reshape(N_TP, hidden_share, D).astype(jnp.float32))
    channel_part = lax.optimization_barrier(channel_part.astype(jnp.bfloat16)).astype(jnp.float32)
    return (middle_full + lax.optimization_barrier(jnp.sum(channel_part, axis=0))).astype(jnp.bfloat16)
```

```python
import functools
import math

import jax
import jax.numpy as jnp
from jax import lax
from jax.experimental import pallas as pl
from jax.experimental.pallas import tpu as pltpu
from jax.sharding import PartitionSpec as P

NOPE_W = 128
NOPE_N = 64
LANES = 128
MESH = pl.DeviceIdType.MESH
BF = jnp.bfloat16
F32 = jnp.float32

rope_base = 10000.0
norm_eps = 1e-06


def cut_points(tiles, parts):
    plain = [k * tiles // parts for k in range(parts + 1)]
    even = [
        k * tiles // parts if 2 * k <= parts else tiles - (parts - k) * tiles // parts
        for k in range(parts + 1)
    ]

    def widest(cuts):
        return max(b - a for a, b in zip(cuts, cuts[1:]))

    return even if widest(even) <= widest(plain) else plain


def dot(a, b):
    return jnp.dot(a, b, preferred_element_type=F32)


def dot_t(a, b):
    return lax.dot_general(a, b, (((1,), (1,)), ((), ())), preferred_element_type=F32)


def layer_kernel(
    n,
    lat_in, qw, qn, gain, taps,
    x_in, kuw, kun, vuw, vun, ow, on, gate, value, down,
    out,
    lat, kuw_v, kun_v, vuw_v, vun_v, ow_v, xin_v,
    kw, kn, vw, vn, att, hpb, hrecv, mid,
    wg, wv, wd, xs, gp, vp, edge, halo, hid, pb, xr, zin,
    loc,
    lz_s, lz_r, lx_s, lx_r, lc_s, lc_r, lo_s, lo_r,
    wz_s, wz_r, wy_s, wy_r, wc_s, wc_r, wl,
    hx_s, hx_r, azr_s, azl_s, az_r, ax_s, ax_r, e_s, e_r,
    rx_s, rx_r, rz_s, rz_r,
):
    G, S, T = n["G"], n["S"], n["T"]
    Z = S // 2
    R = lat_in.shape[0]
    B = R // T
    LW = kuw.shape[0]
    D = xs.shape[3]
    HW, HN = qw.shape[0], qn.shape[0]
    WMAX = wg.shape[3]
    depth = gate.shape[0]
    cuts = cut_points(gate.shape[1] // LANES, Z)
    widths = [(b - a) * LANES for a, b in zip(cuts, cuts[1:])]
    g, s, t = lax.axis_index("grp"), lax.axis_index("sp"), lax.axis_index("tp")
    z, c = s // 2, s % 2

    def zdev(zz):
        return (g, 2 * zz + c, t)

    def xdev(tt):
        return (g, s, tt)

    sib = (g, 2 * z + 1 - c, t)
    xpart = [(t + d) % T for d in range(1, T)]
    if n["share"]:
        pb = xs

    def slot(sender, receiver):
        return (sender - receiver + T) % T - 1

    ypart = [(g + d) % G for d in range(1, G)]

    def rcopy(src, dst, ss, rs, dev):
        return pltpu.make_async_remote_copy(
            src_ref=src, dst_ref=dst, send_sem=ss, recv_sem=rs, device_id=dev, device_id_type=MESH
        )

    def got(ref, rs):
        rcopy(ref, ref, rs, rs, sib).wait_recv()

    def sent(ref, ss):
        rcopy(ref, ref, ss, ss, sib).wait_send()

    def rows(part):
        return pl.ds(pl.multiple_of(part * B, B), B)

    bar = pltpu.get_barrier_semaphore()
    for zz in range(Z):
        @pl.when(zz != z)
        def _():
            pl.semaphore_signal(bar, inc=1, device_id=zdev(zz), device_id_type=MESH)
    for tt in xpart:
        pl.semaphore_signal(bar, inc=1, device_id=xdev(tt), device_id_type=MESH)
    for gg in ypart:
        pl.semaphore_signal(bar, inc=1, device_id=(gg, s, t), device_id_type=MESH)
    pl.semaphore_signal(bar, inc=1, device_id=sib, device_id_type=MESH)
    pl.semaphore_wait(bar, Z + T + G - 2)

    for zz in range(Z):
        @pl.when(zz != z)
        def _():
            rcopy(lat_in.at[rows(t)], lat.at[s, rows(t)], lz_s.at[zz], lz_r.at[z], zdev(zz)).start()
    rcopy(lat_in, lat.at[s], lo_s, lo_r, sib).start()

    mats = ((gate, wg), (value, wv), (down, wd))
    hd = depth // G

    def piece(ai, zz, cc, gg, w):
        if ai < 2:
            return mats[ai][1].at[zz, cc, pl.ds(pl.multiple_of(gg * hd, hd), hd), pl.ds(0, w)]
        wh = w // G
        return wd.at[zz, cc, pl.ds(pl.multiple_of(gg * wh, wh), wh)]

    def slab(ai, cc, w):
        if ai < 2:
            return mats[ai][1].at[:, cc, :, pl.ds(0, w)]
        return wd.at[:, cc, pl.ds(0, w)]

    def own_copy(ai, zz):
        w, lo = widths[zz], cuts[zz] * LANES
        if ai < 2:
            return pltpu.make_async_copy(
                mats[ai][0].at[:, pl.ds(lo, w)], mats[ai][1].at[zz, c, :, pl.ds(0, w)], wl.at[ai]
            )
        return pltpu.make_async_copy(down.at[pl.ds(lo, w)], wd.at[zz, c, pl.ds(0, w)], wl.at[ai])

    def hbm_piece(ai, zz):
        w, lo = widths[zz], cuts[zz] * LANES
        if ai < 2:
            return mats[ai][0].at[pl.ds(pl.multiple_of(g * hd, hd), hd), pl.ds(lo, w)]
        wh = w // G
        return down.at[pl.ds(pl.multiple_of(lo + g * wh, math.gcd(lo, wh) if lo else wh), wh)]

    def spread(ai):
        for zz in range(Z):
            if widths[zz]:
                @pl.when(zz != z)
                def _():
                    rcopy(
                        hbm_piece(ai, zz), piece(ai, z, c, g, widths[zz]),
                        wz_s.at[ai, zz], wz_r.at[ai, z], zdev(zz),
                    ).start()

                @pl.when(zz == z)
                def _():
                    own_copy(ai, zz).start()

    def by_width(body):
        for w in sorted(set(widths)):
            mine = functools.reduce(
                jnp.logical_or, [z == k for k in range(Z) if widths[k] == w]
            )

            @pl.when(mine)
            def _():
                body(w)

    def relay_y(ai):
        def body(w):
            if not w:
                return
            for zz in range(Z):
                @pl.when(zz != z)
                def _():
                    part = piece(ai, zz, c, g, w)
                    got(part, wz_r.at[ai, zz])
                    for gg in ypart:
                        rcopy(part, part, wy_s.at[ai, zz, gg], wy_r.at[ai, zz, g], (gg, s, t)).start()
        by_width(body)

    def relay_core(ai):
        def body(w):
            if not w:
                return
            for zz in range(Z):
                if widths[zz] == w:
                    @pl.when(zz == z)
                    def _():
                        own_copy(ai, zz).wait()
            for zz in range(Z):
                @pl.when(zz != z)
                def _():
                    for gg in ypart:
                        got(piece(ai, zz, c, gg, w), wy_r.at[ai, zz, gg])
            rcopy(slab(ai, c, w), slab(ai, c, w), wc_s.at[ai], wc_r.at[ai], sib).start()
        by_width(body)

    def arrive(ai):
        def body(w):
            if w:
                got(slab(ai, 1 - c, w), wc_r.at[ai])
        by_width(body)

    def spread_sent(ai):
        for zz in range(Z):
            if widths[zz]:
                @pl.when(zz != z)
                def _():
                    sent(hbm_piece(ai, zz), wz_s.at[ai, zz])

        def body(w):
            if not w:
                return
            for zz in range(Z):
                @pl.when(zz != z)
                def _():
                    for gg in ypart:
                        sent(piece(ai, zz, c, g, w), wy_s.at[ai, zz, gg])
            sent(slab(ai, c, w), wc_s.at[ai])
        by_width(body)

    for ai in range(3):
        spread(ai)

    half = NOPE_N
    local = [
        pltpu.make_async_copy(kuw, kuw_v, loc.at[0]),
        pltpu.make_async_copy(kun, kun_v, loc.at[1]),
        pltpu.make_async_copy(vuw, vuw_v, loc.at[2]),
        pltpu.make_async_copy(vun, vun_v, loc.at[3]),
        pltpu.make_async_copy(x_in, xin_v, loc.at[4]),
        pltpu.make_async_copy(ow, ow_v.at[pl.ds(0, HW * LANES)], loc.at[5]),
    ]
    for h in range(HN):
        local.append(
            pltpu.make_async_copy(
                on.at[pl.ds(h * half, half)],
                ow_v.at[pl.ds((HW + h) * LANES, half)],
                loc.at[6 + h],
            )
        )
    for cp in local:
        cp.start()
    for h in range(HN):
        ow_v[pl.ds((HW + h) * LANES + half, LANES - half), :] = jnp.zeros((LANES - half, D), BF)

    def clear(w):
        if w < WMAX:
            gap = WMAX - w
            for ref in (wg, wv):
                ref[:, :, :, pl.ds(w, gap)] = jnp.zeros((Z, 2, depth, gap), BF)
            wd[:, :, pl.ds(w, gap), :] = jnp.zeros((Z, 2, gap, wd.shape[3]), BF)
    by_width(clear)

    lat[s] = lat_in[...]
    for cp in local[:4]:
        cp.wait()

    for zz in range(Z):
        @pl.when(zz != z)
        def _():
            part = lat.at[2 * zz + c, rows(t)]
            got(part, lz_r.at[zz])
            for tt in xpart:
                rcopy(part, part, lx_s.at[zz, tt], lx_r.at[zz, t], xdev(tt)).start()
            rcopy(part, part, lc_s.at[zz, t], lc_r.at[zz, t], sib).start()
    for zz in range(Z):
        @pl.when(zz != z)
        def _():
            for tt in xpart:
                part = lat.at[2 * zz + c, rows(tt)]
                got(part, lx_r.at[zz, tt])
                rcopy(part, part, lc_s.at[zz, tt], lc_r.at[zz, tt], sib).start()
    got(lat.at[2 * z + 1 - c], lo_r)
    for zz in range(Z):
        @pl.when(zz != z)
        def _():
            for tt in range(T):
                got(lat.at[2 * zz + 1 - c, rows(tt)], lc_r.at[zz, tt])

    def expand(i, carry):
        at = pl.ds(pl.multiple_of(i * R, R), R)
        low = lat[i, :, pl.ds(0, LW)]
        turned = lat[i, :, pl.ds(LW, LANES)]
        key = dot(low, kuw_v[...]).astype(BF)
        val = dot(low, vuw_v[...]).astype(BF)
        for h in range(HW):
            kw[h, at, pl.ds(0, LANES)] = key[:, h * LANES : (h + 1) * LANES]
            kw[h, at, pl.ds(LANES, LANES)] = turned
            vw[h, at, :] = val[:, h * LANES : (h + 1) * LANES]
        key = dot(low, kun_v[...]).astype(BF)
        val = dot(low, vun_v[...]).astype(BF)
        for h in range(HN):
            kn[h, at, :] = key[:, h * LANES : (h + 1) * LANES] + turned
            vn[h, at, :] = val[:, h * LANES : (h + 1) * LANES]
        return carry

    lax.fori_loop(0, S, expand, 0)

    def heads(q, k, v, count, first, scale):
        def body(h, carry):
            score = dot_t(q[h], k[h]) * (scale * math.log2(math.e))
            prob = jnp.exp2(score - jnp.max(score, axis=-1, keepdims=True))
            total = jnp.sum(prob, axis=-1, keepdims=True)
            mixed = dot(prob.astype(BF), v[h]) / total
            at = pl.ds(pl.multiple_of((first + h) * LANES, LANES), LANES)
            att[:, at] = mixed.astype(BF)
            return carry

        lax.fori_loop(0, count, body, 0)

    heads(qw, kw, vw, HW, 0, n["scale_w"])
    relay_y(0)
    heads(qn, kn, vn, HN, HW, n["scale_n"])

    for cp in local[4:]:
        cp.wait()
    NB = n["NB"]
    cw = D // NB
    for j in range(NB):
        cols = pl.ds(j * cw, cw)
        hpb[:, cols] = dot(att[...], ow_v[:, cols]).astype(BF)
        for tt in xpart:
            rcopy(
                hpb.at[rows(tt), cols], hrecv.at[t, :, cols], hx_s.at[tt, j], hx_r.at[t, j], xdev(tt)
            ).start()
    for j in range(NB):
        cols = pl.ds(j * cw, cw)
        part = hpb[rows(t), cols].astype(F32)
        for tt in xpart:
            got(hrecv.at[tt, :, cols], hx_r.at[tt, j])
            part = part + hrecv[tt, :, cols].astype(F32)
        mid[:, cols] = (xin_v[:, cols].astype(F32) + part).astype(BF).astype(F32)
    full = mid[...]
    power = jnp.mean(full * full, axis=-1, keepdims=True)
    xs[z, t] = (full * lax.rsqrt(power + norm_eps) * gain[...]).astype(BF)

    def forward(zi):
        blk = xs.at[zi, t]

        @pl.when((zi <= z) & (z < Z - 1))
        def _():
            rcopy(blk, blk, azr_s.at[zi], az_r.at[zi], zdev(z + 1)).start()

        @pl.when((zi >= z) & (z > 0))
        def _():
            rcopy(blk, blk, azl_s.at[zi], az_r.at[zi], zdev(z - 1)).start()
        for tt in xpart:
            rcopy(blk, blk, ax_s.at[zi, tt], ax_r.at[zi, t], xdev(tt)).start()

    def rows_sent():
        for zz in range(Z):
            @pl.when((zz <= z) & (z < Z - 1))
            def _():
                sent(xs.at[zz, t], azr_s.at[zz])

            @pl.when((zz >= z) & (z > 0))
            def _():
                sent(xs.at[zz, t], azl_s.at[zz])
            for tt in xpart:
                sent(xs.at[zz, t], ax_s.at[zz, tt])

    near = jnp.minimum(z, Z - 1 - z)
    outward = jnp.where(z < Z - 1 - z, 1, -1)

    def order(i):
        sign = jnp.where(i % 2 == 1, 1, -1)
        return jnp.where(i <= 2 * near, z + sign * ((i + 1) // 2), z + outward * (i - near))

    forward(z)
    relay_y(1)
    relay_core(0)
    relay_y(2)
    arrive(0)
    relay_core(1)
    arrive(1)

    NC = WMAX // n["NW"]

    def project(i, carry):
        zi = order(i)

        @pl.when(i + 1 < Z)
        def _():
            nxt = order(i + 1)
            got(xs.at[nxt, t], az_r.at[nxt])
            forward(nxt)
        for tt in xpart:
            got(xs.at[zi, tt], ax_r.at[zi, tt])
        block = xs[zi].reshape(R, D)
        for j in range(n["NW"]):
            cols = pl.ds(j * NC, NC)
            pre = dot(block, wg[:, :, :, cols].reshape(D, NC)).astype(BF)
            gp[zi, :, cols] = pre
            edge[zi, pl.ds(0, 8), cols] = pre[:8].astype(F32)
            edge[zi, pl.ds(8, 8), cols] = pre[R - 8 :].astype(F32)
        for j in range(n["NW"]):
            cols = pl.ds(j * NC, NC)
            vp[zi, :, cols] = dot(block, wv[:, :, :, cols].reshape(D, NC))
        return carry

    lax.fori_loop(0, Z, project, 0)
    rcopy(edge, halo, e_s, e_r, sib).start()
    relay_core(2)
    arrive(2)
    got(halo, e_r)
    if n["share"]:
        rows_sent()

    place = lax.broadcasted_iota(jnp.int32, (R, NC), 0)
    OW = wd.shape[3]

    def add_up(zi):
        total = pb[zi, t].astype(F32)
        for tt in xpart:
            part = xr.at[zi, slot(tt, t)]
            got(part, rx_r.at[zi, tt])
            total = total + part[...].astype(F32)
        inner = ((zi > z) & (z > 0)) | ((zi < z) & (z < Z - 1))

        @pl.when(inner)
        def _():
            got(zin.at[zi], rz_r.at[zi])
            pb[zi, t] = (total + zin[zi].astype(F32)).astype(BF)

        @pl.when(jnp.logical_not(inner))
        def _():
            pb[zi, t] = total.astype(BF)

        @pl.when(zi > z)
        def _():
            rcopy(pb.at[zi, t], zin.at[zi], rz_s.at[zi], rz_r.at[zi], zdev(z + 1)).start()

        @pl.when(zi < z)
        def _():
            into = jnp.where(zi == z - 1, Z, zi)
            rcopy(pb.at[zi, t], zin.at[into], rz_s.at[zi], rz_r.at[into], zdev(z - 1)).start()

    def mix(k, carry):
        zi = order(Z - 1 - k)
        above, below = zi - 1 + c, zi + c
        has_above = jnp.where(above >= 0, 1.0, 0.0)
        has_below = jnp.where(below < Z, 1.0, 0.0)
        above, below = jnp.maximum(above, 0), jnp.minimum(below, Z - 1)
        for j in range(n["NW"]):
            cols = pl.ds(j * NC, NC)
            pre = gp[zi, :, cols].astype(F32)
            prev = halo[above, pl.ds(8, 8), cols][7:8] * has_above
            post = halo[below, pl.ds(0, 8), cols][0:1] * has_below
            up = jnp.where(place == 0, prev, pltpu.roll(pre, 1, 0))
            dn = jnp.where(place == R - 1, post, pltpu.roll(pre, R - 1, 0))
            conv = taps[0:1, cols] * up + taps[1:2, cols] * pre + taps[2:3, cols] * dn
            hid[:, cols] = (conv / (1.0 + jnp.exp(-conv)) * vp[zi, :, cols]).astype(BF)
        for zz in range(Z):
            for cc in range(2):
                part = dot(hid[...], wd[zz, cc]).astype(BF)
                pb[zi, :, :, pl.ds((2 * zz + cc) * OW, OW)] = part.reshape(T, B, OW)
        for tt in xpart:
            rcopy(pb.at[zi, tt], xr.at[zi, slot(t, tt)], rx_s.at[zi, tt], rx_r.at[zi, t], xdev(tt)).start()

        @pl.when(k > 0)
        def _():
            add_up(order(Z - k))
        return carry

    lax.fori_loop(0, Z, mix, 0)
    total = pb[z, t].astype(F32)
    for tt in xpart:
        part = xr.at[z, slot(tt, t)]
        got(part, rx_r.at[z, tt])
        total = total + part[...].astype(F32)
    mid[...] = mid[...] + total

    @pl.when(z > 0)
    def _():
        got(zin.at[z], rz_r.at[z])
        mid[...] = mid[...] + zin[z].astype(F32)

    @pl.when(z < Z - 1)
    def _():
        got(zin.at[Z], rz_r.at[Z])
        mid[...] = mid[...] + zin[Z].astype(F32)
    out[...] = mid[...].astype(BF)

    sent(lat_in, lo_s)
    sent(edge, e_s)
    for ai in range(3):
        spread_sent(ai)
    for tt in xpart:
        for j in range(NB):
            sent(hpb.at[rows(tt), pl.ds(j * cw, cw)], hx_s.at[tt, j])
    for zz in range(Z):
        @pl.when(zz != z)
        def _():
            part = lat.at[2 * zz + c, rows(t)]
            sent(part, lz_s.at[zz])
            for tt in xpart:
                sent(part, lx_s.at[zz, tt])
            for tt in range(T):
                sent(part, lc_s.at[zz, tt])
            sent(pb.at[zz, t], rz_s.at[zz])
        for tt in xpart:
            sent(pb.at[zz, tt], rx_s.at[zz, tt])
    if not n["share"]:
        rows_sent()


def rope_tables(row_start, row_total, span_width):
    places = (row_start + jnp.arange(row_total, dtype=jnp.int32)).astype(F32)
    frequency = jnp.power(
        rope_base, -jnp.arange(0, span_width, 2, dtype=jnp.int32).astype(F32) / span_width
    )
    angles = places[:, None] * frequency[None, :]
    angles = jnp.concatenate([angles, angles], axis=-1)
    return (jnp.cos(angles), jnp.sin(angles))


def spin_rows(entries, cosine, sine_table):
    entries = entries.astype(F32)
    lead_half, tail_half = jnp.split(entries, 2, axis=-1)
    return entries * cosine + jnp.concatenate([-tail_half, lead_half], axis=-1) * sine_table


def split_queries(queries, heads, nope, cosine, sine_table):
    shaped = queries.reshape(queries.shape[0], heads, -1)
    turned = spin_rows(shaped[:, :, nope:], cosine[:, None, :], sine_table[:, None, :]).astype(BF)
    return shaped[:, :, :nope], turned


def layer(
    layer_input,
    latent,
    rope_key,
    query_wide,
    query_narrow,
    key_up_wide,
    value_up_wide,
    key_up_narrow,
    value_up_narrow,
    out_wide,
    out_narrow,
    norm_gain,
    gate_weight,
    value_weight,
    conv_weight,
    down_weight,
):
    G, S, T = lax.axis_size("grp"), lax.axis_size("sp"), lax.axis_size("tp")
    Z = S // 2
    R, LW = latent.shape
    rot = rope_key.shape[1]
    D = layer_input.shape[1]
    B = R // T
    HW = key_up_wide.shape[1] // NOPE_W
    HN = key_up_narrow.shape[1] // NOPE_N
    cosine, sine_table = rope_tables(lax.axis_index("sp") * R, R, rot)
    turned_key = spin_rows(rope_key, cosine, sine_table).astype(BF)
    lat = jnp.concatenate([latent, turned_key, jnp.zeros((R, LANES - rot), BF)], axis=1)
    nope, turned = split_queries(query_wide, HW, NOPE_W, cosine, sine_table)
    qw = jnp.concatenate([nope, turned, jnp.zeros((R, HW, LANES - rot), BF)], axis=2)
    nope, turned = split_queries(query_narrow, HN, NOPE_N, cosine, sine_table)
    qn = jnp.concatenate([turned, nope], axis=2)
    qw, qn = qw.transpose(1, 0, 2), qn.transpose(1, 0, 2)
    pad_key = jnp.pad(
        key_up_narrow.reshape(LW, HN, NOPE_N), ((0, 0), (0, 0), (LANES - NOPE_N, 0))
    ).reshape(LW, HN * LANES)
    pad_value = jnp.pad(
        value_up_narrow.reshape(LW, HN, NOPE_N), ((0, 0), (0, 0), (0, LANES - NOPE_N))
    ).reshape(LW, HN * LANES)
    tiles = gate_weight.shape[1] // LANES
    cuts = cut_points(tiles, Z)
    wmax = max(b - a for a, b in zip(cuts, cuts[1:])) * LANES
    start = jnp.asarray(cuts, jnp.int32)[lax.axis_index("sp") // 2] * LANES
    taps = lax.dynamic_slice_in_dim(
        jnp.pad(conv_weight, ((0, 0), (0, wmax))), start, wmax, axis=1
    )
    keys = S * R
    depth, ow = gate_weight.shape[0], down_weight.shape[1]
    share = Z * T * B * D * 2 > 8 << 20
    n = dict(
        share=share,
        G=G,
        S=S,
        T=T,
        NB=4,
        NW=max(1, wmax // 256),
        scale_w=1.0 / math.sqrt(NOPE_W + rot),
        scale_n=1.0 / math.sqrt(NOPE_N + rot),
    )
    vmem = pl.BlockSpec(memory_space=pltpu.VMEM)
    hbm = pl.BlockSpec(memory_space=pl.ANY)

    def V(*shape, dtype=BF):
        return pltpu.VMEM(shape, dtype)

    def sem(*shape):
        return pltpu.SemaphoreType.DMA(shape)

    one = pltpu.SemaphoreType.DMA
    scratch = [
        V(S, R, lat.shape[1]),
        V(LW, HW * LANES), V(LW, HN * LANES), V(LW, HW * LANES), V(LW, HN * LANES),
        V((HW + HN) * LANES, D), V(B, D),
        V(HW, keys, 2 * LANES), V(HN, keys, LANES), V(HW, keys, LANES), V(HN, keys, LANES),
        V(R, (HW + HN) * LANES), V(R, D), V(T, B, D), V(B, D, dtype=F32),
        V(Z, 2, depth, wmax), V(Z, 2, depth, wmax), V(Z, 2, wmax, ow),
        V(Z, T, B, D), V(Z, R, wmax), V(Z, R, wmax, dtype=F32),
        V(Z, 16, wmax, dtype=F32), V(Z, 16, wmax, dtype=F32), V(R, wmax),
        V(8, LANES) if share else V(Z, T, B, D), V(Z, T - 1, B, D), V(Z + 1, B, D),
        sem(6 + HN),
        sem(Z), sem(Z), sem(Z, T), sem(Z, T), sem(Z, T), sem(Z, T), one, one,
        sem(3, Z), sem(3, Z), sem(3, Z, G), sem(3, Z, G), sem(3), sem(3), sem(3),
        sem(T, 4), sem(T, 4), sem(Z), sem(Z), sem(Z), sem(Z, T), sem(Z, T), one, one,
        sem(Z, T), sem(Z, T), sem(Z), sem(Z + 1),
    ]
    return pl.pallas_call(
        functools.partial(layer_kernel, n),
        out_shape=jax.ShapeDtypeStruct((B, D), BF),
        in_specs=[vmem] * 5 + [hbm] * 10,
        out_specs=vmem,
        scratch_shapes=scratch,
        compiler_params=pltpu.CompilerParams(
            collective_id=0, has_side_effects=True, vmem_limit_bytes=63 << 20
        ),
        name="layer",
    )(
        lat, qw, qn, norm_gain.reshape(1, D), taps,
        layer_input, key_up_wide, pad_key, value_up_wide, pad_value, out_wide, out_narrow,
        gate_weight, value_weight, down_weight,
    )


def solution(mesh):
    in_specs = (
        P(("grp", "sp", "tp"), None),
        P(("grp", "sp"), None),
        P(("grp", "sp"), None),
        P(("grp", "sp"), "tp"),
        P(("grp", "sp"), "tp"),
        P(None, "tp"),
        P(None, "tp"),
        P(None, "tp"),
        P(None, "tp"),
        P("tp", None),
        P("tp", None),
        P(),
        P("sp", "tp"),
        P("sp", "tp"),
        P(None, "tp"),
        P("tp", "sp"),
    )
    out_specs = P(("grp", "sp", "tp"), None)
    return jax.shard_map(
        layer, mesh=mesh, in_specs=in_specs, out_specs=out_specs, check_vma=False
    )
```

```python
import functools
import math

import jax
import jax.numpy as jnp
from jax import lax
from jax.experimental import pallas as pl
from jax.experimental.pallas import tpu as pltpu
from jax.sharding import PartitionSpec as P

NOPE_W = 128
NOPE_N = 64
LANES = 128
MESH = pl.DeviceIdType.MESH
BF = jnp.bfloat16
F32 = jnp.float32

rope_base = 10000.0
norm_eps = 1e-06


def cut_points(tiles, parts):
    plain = [k * tiles // parts for k in range(parts + 1)]
    even = [
        k * tiles // parts if 2 * k <= parts else tiles - (parts - k) * tiles // parts
        for k in range(parts + 1)
    ]

    def widest(cuts):
        return max(b - a for a, b in zip(cuts, cuts[1:]))

    return even if widest(even) <= widest(plain) else plain


def dot(a, b):
    return jnp.dot(a, b, preferred_element_type=F32)


def dot_t(a, b):
    return lax.dot_general(a, b, (((1,), (1,)), ((), ())), preferred_element_type=F32)


def layer_kernel(
    n,
    latent, rope, query_w, query_n, trig, gain,
    x_in, kuw, kun, vuw, vun, ow, on, conv, gate, value, down,
    out,
    lat, kuw_v, kun_v, vuw_v, vun_v, ow_v, xin_v,
    taps, qw, qn, kw, kn, vw, vn, att, hpb, hrecv, mid,
    wg, wv, wd, xs, gp, vp, edge, halo, hid, pb, xr, zin,
    loc,
    lz_s, lz_r, lx_s, lx_r, lc_s, lc_r, lo_s, lo_r,
    wz_s, wz_r, wy_s, wy_r, wc_s, wc_r, wl,
    hx_s, hx_r, azr_s, azl_s, az_r, ax_s, ax_r, e_s, e_r,
    rx_s, rx_r, rz_s, rz_r,
):
    G, S, T = n["G"], n["S"], n["T"]
    Z = S // 2
    R = latent.shape[0]
    B = R // T
    LW = kuw.shape[0]
    D = xs.shape[3]
    HW, HN = qw.shape[0], qn.shape[0]
    WMAX = wg.shape[3]
    depth = gate.shape[0]
    cuts = cut_points(gate.shape[1] // LANES, Z)
    widths = [(b - a) * LANES for a, b in zip(cuts, cuts[1:])]
    g, s, t = lax.axis_index("grp"), lax.axis_index("sp"), lax.axis_index("tp")
    z, c = s // 2, s % 2

    def zdev(zz):
        return (g, 2 * zz + c, t)

    def xdev(tt):
        return (g, s, tt)

    sib = (g, 2 * z + 1 - c, t)
    xpart = [(t + d) % T for d in range(1, T)]
    if n["share"]:
        pb = xs

    def slot(sender, receiver):
        return (sender - receiver + T) % T - 1

    ypart = [(g + d) % G for d in range(1, G)]

    def rcopy(src, dst, ss, rs, dev):
        return pltpu.make_async_remote_copy(
            src_ref=src, dst_ref=dst, send_sem=ss, recv_sem=rs, device_id=dev, device_id_type=MESH
        )

    def got(ref, rs):
        rcopy(ref, ref, rs, rs, sib).wait_recv()

    def sent(ref, ss):
        rcopy(ref, ref, ss, ss, sib).wait_send()

    def rows(part):
        return pl.ds(pl.multiple_of(part * B, B), B)

    def by_lane(first, second, width):
        lane = lax.broadcasted_iota(jnp.int32, (R, LANES), 1)
        return jnp.where(lane < width, first, second)

    def turn(entries):
        turned = by_lane(-pltpu.roll(entries, LANES - 32, 1), pltpu.roll(entries, 32, 1), 32)
        return entries * trig[0] + turned * trig[1]

    local = [
        pltpu.make_async_copy(kuw, kuw_v, loc.at[0]),
        pltpu.make_async_copy(kun, kun_v, loc.at[1]),
        pltpu.make_async_copy(vuw, vuw_v, loc.at[2]),
        pltpu.make_async_copy(vun, vun_v, loc.at[3]),
        pltpu.make_async_copy(x_in, xin_v, loc.at[4]),
        pltpu.make_async_copy(ow, ow_v.at[pl.ds(0, HW * LANES)], loc.at[5]),
        pltpu.make_async_copy(on, ow_v.at[pl.ds(HW * LANES, HN * NOPE_N)], loc.at[6]),
    ]
    for cp in local:
        cp.start()
    lat[s, :, pl.ds(0, LW)] = latent[...]
    entries = jnp.concatenate([rope[...].astype(F32), jnp.zeros((R, LANES - rope.shape[1]), F32)], 1)
    lat[s, :, pl.ds(LW, LANES)] = turn(entries).astype(BF)

    bar = pltpu.get_barrier_semaphore()
    for zz in range(Z):
        @pl.when(zz != z)
        def _():
            pl.semaphore_signal(bar, inc=1, device_id=zdev(zz), device_id_type=MESH)
    for tt in xpart:
        pl.semaphore_signal(bar, inc=1, device_id=xdev(tt), device_id_type=MESH)
    for gg in ypart:
        pl.semaphore_signal(bar, inc=1, device_id=(gg, s, t), device_id_type=MESH)
    pl.semaphore_signal(bar, inc=1, device_id=sib, device_id_type=MESH)
    pl.semaphore_wait(bar, Z + T + G - 2)

    for zz in range(Z):
        @pl.when(zz != z)
        def _():
            part = lat.at[s, rows(t)]
            rcopy(part, part, lz_s.at[zz], lz_r.at[z], zdev(zz)).start()
    rcopy(lat.at[s], lat.at[s], lo_s, lo_r, sib).start()

    mats = ((gate, wg), (value, wv), (down, wd))
    hd = depth // G

    def piece(ai, zz, cc, gg, w):
        if ai < 2:
            return mats[ai][1].at[zz, cc, pl.ds(pl.multiple_of(gg * hd, hd), hd), pl.ds(0, w)]
        wh = w // G
        return wd.at[zz, cc, pl.ds(pl.multiple_of(gg * wh, wh), wh)]

    def slab(ai, cc, w):
        if ai < 2:
            return mats[ai][1].at[:, cc, :, pl.ds(0, w)]
        return wd.at[:, cc, pl.ds(0, w)]

    def own_copy(ai, zz):
        w, lo = widths[zz], cuts[zz] * LANES
        if ai < 2:
            return pltpu.make_async_copy(
                mats[ai][0].at[:, pl.ds(lo, w)], mats[ai][1].at[zz, c, :, pl.ds(0, w)], wl.at[ai]
            )
        return pltpu.make_async_copy(down.at[pl.ds(lo, w)], wd.at[zz, c, pl.ds(0, w)], wl.at[ai])

    def tap_copy(zz):
        w = widths[zz]
        return pltpu.make_async_copy(
            conv.at[:, pl.ds(cuts[zz] * LANES, w)], taps.at[:, pl.ds(0, w)], loc.at[7]
        )

    def hbm_piece(ai, zz):
        w, lo = widths[zz], cuts[zz] * LANES
        if ai < 2:
            return mats[ai][0].at[pl.ds(pl.multiple_of(g * hd, hd), hd), pl.ds(lo, w)]
        wh = w // G
        return down.at[pl.ds(pl.multiple_of(lo + g * wh, math.gcd(lo, wh) if lo else wh), wh)]

    def spread(ai):
        for zz in range(Z):
            if widths[zz]:
                @pl.when(zz != z)
                def _():
                    rcopy(
                        hbm_piece(ai, zz), piece(ai, z, c, g, widths[zz]),
                        wz_s.at[ai, zz], wz_r.at[ai, z], zdev(zz),
                    ).start()

                @pl.when(zz == z)
                def _():
                    own_copy(ai, zz).start()

    def by_width(body):
        for w in sorted(set(widths)):
            mine = functools.reduce(
                jnp.logical_or, [z == k for k in range(Z) if widths[k] == w]
            )

            @pl.when(mine)
            def _():
                body(w)

    def relay_y(ai):
        def body(w):
            if not w:
                return
            for zz in range(Z):
                @pl.when(zz != z)
                def _():
                    part = piece(ai, zz, c, g, w)
                    got(part, wz_r.at[ai, zz])
                    for gg in ypart:
                        rcopy(part, part, wy_s.at[ai, zz, gg], wy_r.at[ai, zz, g], (gg, s, t)).start()
        by_width(body)

    def relay_core(ai):
        def body(w):
            if not w:
                return
            for zz in range(Z):
                if widths[zz] == w:
                    @pl.when(zz == z)
                    def _():
                        own_copy(ai, zz).wait()
            for zz in range(Z):
                @pl.when(zz != z)
                def _():
                    for gg in ypart:
                        got(piece(ai, zz, c, gg, w), wy_r.at[ai, zz, gg])
            rcopy(slab(ai, c, w), slab(ai, c, w), wc_s.at[ai], wc_r.at[ai], sib).start()
        by_width(body)

    def arrive(ai):
        def body(w):
            if w:
                got(slab(ai, 1 - c, w), wc_r.at[ai])
        by_width(body)

    def spread_sent(ai):
        for zz in range(Z):
            if widths[zz]:
                @pl.when(zz != z)
                def _():
                    sent(hbm_piece(ai, zz), wz_s.at[ai, zz])

        def body(w):
            if not w:
                return
            for zz in range(Z):
                @pl.when(zz != z)
                def _():
                    for gg in ypart:
                        sent(piece(ai, zz, c, g, w), wy_s.at[ai, zz, gg])
            sent(slab(ai, c, w), wc_s.at[ai])
        by_width(body)

    spread(0)
    spread(1)

    for zz in range(Z):
        if widths[zz]:
            @pl.when(zz == z)
            def _():
                tap_copy(zz).start()

    def clear(w):
        if w < WMAX:
            gap = WMAX - w
            for ref in (wg, wv):
                ref[:, :, :, pl.ds(w, gap)] = jnp.zeros((Z, 2, depth, gap), BF)
            wd[:, :, pl.ds(w, gap), :] = jnp.zeros((Z, 2, gap, wd.shape[3]), BF)
            taps[:, pl.ds(w, gap)] = jnp.zeros((taps.shape[0], gap), F32)
    by_width(clear)

    for h in range(0, HW, 2):
        one, two, three = (
            query_w[:, pl.ds((3 * (h // 2) + i) * LANES, LANES)].astype(F32) for i in range(3)
        )
        two_r, three_r = pltpu.roll(two, 64, 1), pltpu.roll(three, 64, 1)
        qw[h, :, pl.ds(0, LANES)] = one.astype(BF)
        qw[h, :, pl.ds(LANES, LANES)] = turn(two).astype(BF)
        qw[h + 1, :, pl.ds(0, LANES)] = by_lane(two_r, three_r, 64).astype(BF)
        qw[h + 1, :, pl.ds(LANES, LANES)] = turn(three_r).astype(BF)
    for h in range(HN):
        entries = pltpu.roll(query_n[:, pl.ds(h * LANES, LANES)].astype(F32), 64, 1)
        qn[h] = by_lane(turn(entries), entries, 64).astype(BF)
    for cp in local[:4]:
        cp.wait()

    def expand(i):
        at = pl.ds(pl.multiple_of(i * R, R), R)
        low = lat[i, :, pl.ds(0, LW)]
        turned = lat[i, :, pl.ds(LW, LANES)]
        key = dot(low, kuw_v[...]).astype(BF)
        val = dot(low, vuw_v[...]).astype(BF)
        for h in range(HW):
            kw[h, at, pl.ds(0, LANES)] = key[:, h * LANES : (h + 1) * LANES]
            kw[h, at, pl.ds(LANES, LANES)] = turned
            vw[h, at, :] = val[:, h * LANES : (h + 1) * LANES]
        key = dot(low, kun_v[...]).astype(BF).astype(F32)
        val = dot(low, vun_v[...]).astype(BF)
        turned = turned.astype(F32)
        for h in range(0, HN, 2):
            pair = key[:, h * NOPE_N : h * NOPE_N + LANES]
            kn[h, at, :] = by_lane(turned, pltpu.roll(pair, 64, 1), 64).astype(BF)
            kn[h + 1, at, :] = by_lane(turned, pair, 64).astype(BF)
            vn[h // 2, at, :] = val[:, h * NOPE_N : h * NOPE_N + LANES]

    for zz in range(Z):
        @pl.when(zz != z)
        def _():
            part = lat.at[2 * zz + c, rows(t)]
            got(part, lz_r.at[zz])
            for tt in xpart:
                rcopy(part, part, lx_s.at[zz, tt], lx_r.at[zz, t], xdev(tt)).start()
            rcopy(part, part, lc_s.at[zz, t], lc_r.at[zz, t], sib).start()
    expand(s)

    def mine(zz, carry):
        @pl.when(zz != z)
        def _():
            for tt in xpart:
                part = lat.at[2 * zz + c, rows(tt)]
                got(part, lx_r.at[zz, tt])
                rcopy(part, part, lc_s.at[zz, tt], lc_r.at[zz, tt], sib).start()
            expand(2 * zz + c)
        return carry

    lax.fori_loop(0, Z, mine, 0)
    got(lat.at[2 * z + 1 - c], lo_r)
    expand(2 * z + 1 - c)

    def theirs(zz, carry):
        @pl.when(zz != z)
        def _():
            for tt in range(T):
                got(lat.at[2 * zz + 1 - c, rows(tt)], lc_r.at[zz, tt])
            expand(2 * zz + 1 - c)
        return carry

    lax.fori_loop(0, Z, theirs, 0)

    def attend(q, k, v, scale):
        score = dot_t(q, k) * (scale * math.log2(math.e))
        prob = jnp.exp2(score - jnp.max(score, axis=-1, keepdims=True))
        total = jnp.sum(prob, axis=-1, keepdims=True)
        return dot(prob.astype(BF), v) / total

    def wide(h, carry):
        at = pl.ds(pl.multiple_of(h * LANES, LANES), LANES)
        att[:, at] = attend(qw[h], kw[h], vw[h], n["scale_w"]).astype(BF)
        return carry

    def narrow(p, carry):
        at = pl.ds(pl.multiple_of((HW + p) * LANES, LANES), LANES)
        first = attend(qn[2 * p], kn[2 * p], vn[p], n["scale_n"])
        second = attend(qn[2 * p + 1], kn[2 * p + 1], vn[p], n["scale_n"])
        att[:, at] = by_lane(first, second, 64).astype(BF)
        return carry

    lax.fori_loop(0, HW, wide, 0)
    relay_y(0)
    lax.fori_loop(0, HN // 2, narrow, 0)

    for cp in local[4:]:
        cp.wait()
    NB = n["NB"]
    cw = D // NB
    for j in range(NB):
        cols = pl.ds(j * cw, cw)
        hpb[:, cols] = dot(att[...], ow_v[:, cols]).astype(BF)
        for tt in xpart:
            rcopy(
                hpb.at[rows(tt), cols], hrecv.at[slot(t, tt), :, cols], hx_s.at[tt, j], hx_r.at[t, j], xdev(tt)
            ).start()
    for j in range(NB):
        cols = pl.ds(j * cw, cw)
        part = hpb[rows(t), cols].astype(F32)
        for tt in xpart:
            came = hrecv.at[slot(tt, t), :, cols]
            got(came, hx_r.at[tt, j])
            part = part + came[...].astype(F32)
        mid[:, cols] = (xin_v[:, cols].astype(F32) + part).astype(BF).astype(F32)
    full = mid[...]
    power = jnp.mean(full * full, axis=-1, keepdims=True)
    xs[z, t] = (full * lax.rsqrt(power + norm_eps) * gain[...]).astype(BF)

    U = n["U"]
    sub = B // U

    def strip(zi, tt, u):
        return xs.at[zi, tt, pl.ds(u * sub, sub)]

    def forward(zi, u):
        blk = strip(zi, t, u)

        @pl.when((zi <= z) & (z < Z - 1))
        def _():
            rcopy(blk, blk, azr_s.at[zi, u], az_r.at[zi, u], zdev(z + 1)).start()

        @pl.when((zi >= z) & (z > 0))
        def _():
            rcopy(blk, blk, azl_s.at[zi, u], az_r.at[zi, u], zdev(z - 1)).start()
        for tt in xpart:
            rcopy(blk, blk, ax_s.at[zi, tt, u], ax_r.at[zi, t, u], xdev(tt)).start()

    def rows_sent():
        for zz in range(Z):
            for u in range(U):
                @pl.when((zz <= z) & (z < Z - 1))
                def _():
                    sent(strip(zz, t, u), azr_s.at[zz, u])

                @pl.when((zz >= z) & (z > 0))
                def _():
                    sent(strip(zz, t, u), azl_s.at[zz, u])
                for tt in xpart:
                    sent(strip(zz, t, u), ax_s.at[zz, tt, u])

    near = jnp.minimum(z, Z - 1 - z)
    outward = jnp.where(z < Z - 1 - z, 1, -1)

    def order(i):
        sign = jnp.where(i % 2 == 1, 1, -1)
        return jnp.where(i <= 2 * near, z + sign * ((i + 1) // 2), z + outward * (i - near))

    def relay_rows(i):
        nxt = order(i)
        for u in range(U):
            got(strip(nxt, t, u), az_r.at[nxt, u])
            forward(nxt, u)

    for u in range(U):
        forward(z, u)
    relay_y(1)
    if Z > 1:
        relay_rows(1)
    spread(2)
    relay_core(0)
    arrive(0)
    relay_core(1)
    arrive(1)

    NC = WMAX // n["NW"]

    def project(i, carry):
        zi = order(i)

        for tt in xpart:
            for u in range(U):
                got(strip(zi, tt, u), ax_r.at[zi, tt, u])
        block = xs[zi].reshape(R, D)
        for j in range(n["NW"]):
            cols = pl.ds(j * NC, NC)
            pre = dot(block, wg[:, :, :, cols].reshape(D, NC)).astype(BF)
            gp[zi, :, cols] = pre
            edge[zi, pl.ds(0, 8), cols] = pre[:8].astype(F32)
            edge[zi, pl.ds(8, 8), cols] = pre[R - 8 :].astype(F32)
        for j in range(n["NW"]):
            cols = pl.ds(j * NC, NC)
            vp[zi, :, cols] = dot(block, wv[:, :, :, cols].reshape(D, NC)).astype(vp.dtype)

        @pl.when(i + 2 < Z)
        def _():
            relay_rows(i + 2)

        @pl.when(i == max(0, Z - 3))
        def _():
            relay_y(2)
        return carry

    lax.fori_loop(0, Z, project, 0)
    rcopy(edge, halo, e_s, e_r, sib).start()
    relay_core(2)
    arrive(2)
    got(halo, e_r)
    for zz in range(Z):
        if widths[zz]:
            @pl.when(zz == z)
            def _():
                tap_copy(zz).wait()
    if n["share"]:
        rows_sent()

    place = lax.broadcasted_iota(jnp.int32, (R, NC), 0)
    OW = wd.shape[3]

    J = 2
    SJ = S // J
    DJ = D // J

    def summed(zi, j):
        cols = pl.ds(j * DJ, DJ)
        total = pb[zi, t, :, cols].astype(F32)
        for tt in xpart:
            part = xr.at[zi, slot(tt, t), :, cols]
            got(part, rx_r.at[zi, tt, j])
            total = total + part[...].astype(F32)
        return total

    def add_up(zi, j):
        cols = pl.ds(j * DJ, DJ)
        total = summed(zi, j)
        inner = ((zi > z) & (z > 0)) | ((zi < z) & (z < Z - 1))
        mine = pb.at[zi, t, :, cols]

        @pl.when(inner)
        def _():
            got(zin.at[zi, :, cols], rz_r.at[zi, j])
            mine[...] = (total + zin[zi, :, cols].astype(F32)).astype(BF)

        @pl.when(jnp.logical_not(inner))
        def _():
            mine[...] = total.astype(BF)

        @pl.when(zi > z)
        def _():
            rcopy(mine, zin.at[zi, :, cols], rz_s.at[zi, j], rz_r.at[zi, j], zdev(z + 1)).start()

        @pl.when(zi < z)
        def _():
            into = jnp.where(zi == z - 1, Z, zi)
            rcopy(mine, zin.at[into, :, cols], rz_s.at[zi, j], rz_r.at[into, j], zdev(z - 1)).start()

    def mix(k, carry):
        zi = order(Z - 1 - k)
        above, below = zi - 1 + c, zi + c
        has_above = jnp.where(above >= 0, 1.0, 0.0)
        has_below = jnp.where(below < Z, 1.0, 0.0)
        above, below = jnp.maximum(above, 0), jnp.minimum(below, Z - 1)
        for j in range(n["NW"]):
            cols = pl.ds(j * NC, NC)
            pre = gp[zi, :, cols].astype(F32)
            prev = halo[above, pl.ds(8, 8), cols][7:8] * has_above
            post = halo[below, pl.ds(0, 8), cols][0:1] * has_below
            up = jnp.where(place == 0, prev, pltpu.roll(pre, 1, 0))
            dn = jnp.where(place == R - 1, post, pltpu.roll(pre, R - 1, 0))
            conv = taps[0:1, cols] * up + taps[1:2, cols] * pre + taps[2:3, cols] * dn
            hid[:, cols] = (conv / (1.0 + jnp.exp(-conv)) * vp[zi, :, cols].astype(F32)).astype(BF)
        for j in range(J):
            for b in range(j * SJ, j * SJ + SJ):
                part = dot(hid[...], wd[b // 2, b % 2]).astype(BF)
                pb[zi, :, :, pl.ds(b * OW, OW)] = part.reshape(T, B, OW)
            cols = pl.ds(j * DJ, DJ)
            for tt in xpart:
                rcopy(
                    pb.at[zi, tt, :, cols], xr.at[zi, slot(t, tt), :, cols],
                    rx_s.at[zi, tt, j], rx_r.at[zi, t, j], xdev(tt),
                ).start()
        return carry

    lax.fori_loop(0, Z, mix, 0)

    def pass_on(k, carry):
        zi = order(Z - 1 - k)
        for j in range(J):
            add_up(zi, j)
        return carry

    lax.fori_loop(0, Z - 1, pass_on, 0)
    for j in range(J):
        cols = pl.ds(j * DJ, DJ)
        mid[:, cols] = mid[:, cols] + summed(z, j)

        @pl.when(z > 0)
        def _():
            got(zin.at[z, :, cols], rz_r.at[z, j])
            mid[:, cols] = mid[:, cols] + zin[z, :, cols].astype(F32)

        @pl.when(z < Z - 1)
        def _():
            got(zin.at[Z, :, cols], rz_r.at[Z, j])
            mid[:, cols] = mid[:, cols] + zin[Z, :, cols].astype(F32)
    out[...] = mid[...].astype(BF)

    sent(lat.at[s], lo_s)
    sent(edge, e_s)
    for ai in range(3):
        spread_sent(ai)
    for tt in xpart:
        for j in range(NB):
            sent(hpb.at[rows(tt), pl.ds(j * cw, cw)], hx_s.at[tt, j])
    for zz in range(Z):
        @pl.when(zz != z)
        def _():
            part = lat.at[2 * zz + c, rows(t)]
            sent(part, lz_s.at[zz])
            for tt in xpart:
                sent(part, lx_s.at[zz, tt])
            for tt in range(T):
                sent(part, lc_s.at[zz, tt])
            for j in range(J):
                sent(pb.at[zz, t, :, pl.ds(j * DJ, DJ)], rz_s.at[zz, j])
        for tt in xpart:
            for j in range(J):
                sent(pb.at[zz, tt, :, pl.ds(j * DJ, DJ)], rx_s.at[zz, tt, j])
    if not n["share"]:
        rows_sent()


def rope_tables(row_start, row_total, span_width):
    places = (row_start + jnp.arange(row_total, dtype=jnp.int32)).astype(F32)
    frequency = jnp.power(
        rope_base, -jnp.arange(0, span_width, 2, dtype=jnp.int32).astype(F32) / span_width
    )
    angles = places[:, None] * jnp.tile(frequency, 2 * LANES // span_width)[None, :]
    valid = jnp.arange(LANES) < span_width
    return jnp.where(valid, jnp.stack([jnp.cos(angles), jnp.sin(angles)]), 0.0)


def layer(
    layer_input,
    latent,
    rope_key,
    query_wide,
    query_narrow,
    key_up_wide,
    value_up_wide,
    key_up_narrow,
    value_up_narrow,
    out_wide,
    out_narrow,
    norm_gain,
    gate_weight,
    value_weight,
    conv_weight,
    down_weight,
):
    G, S, T = lax.axis_size("grp"), lax.axis_size("sp"), lax.axis_size("tp")
    Z = S // 2
    R, LW = latent.shape
    rot = rope_key.shape[1]
    D = layer_input.shape[1]
    B = R // T
    HW = key_up_wide.shape[1] // NOPE_W
    HN = key_up_narrow.shape[1] // NOPE_N
    trig = rope_tables(lax.axis_index("sp") * R, R, rot)
    tiles = gate_weight.shape[1] // LANES
    cuts = cut_points(tiles, Z)
    wmax = max(b - a for a, b in zip(cuts, cuts[1:])) * LANES
    keys = S * R
    depth, ow = gate_weight.shape[0], down_weight.shape[1]
    U = 2 if B % 32 == 0 else 1
    share = Z * T * B * D * 2 > 8 << 20
    n = dict(
        share=share,
        U=U,
        G=G,
        S=S,
        T=T,
        NB=4,
        NW=max(1, wmax // 256),
        scale_w=1.0 / math.sqrt(NOPE_W + rot),
        scale_n=1.0 / math.sqrt(NOPE_N + rot),
    )
    vmem = pl.BlockSpec(memory_space=pltpu.VMEM)
    hbm = pl.BlockSpec(memory_space=pl.ANY)

    def V(*shape, dtype=BF):
        return pltpu.VMEM(shape, dtype)

    def sem(*shape):
        return pltpu.SemaphoreType.DMA(shape)

    one = pltpu.SemaphoreType.DMA
    scratch = [
        V(S, R, LW + LANES),
        V(*key_up_wide.shape), V(*key_up_narrow.shape),
        V(*value_up_wide.shape), V(*value_up_narrow.shape),
        V(HW * LANES + HN * NOPE_N, D), V(B, D), V(conv_weight.shape[0], wmax, dtype=F32),
        V(HW, R, 2 * LANES), V(HN, R, LANES),
        V(HW, keys, 2 * LANES), V(HN, keys, LANES), V(HW, keys, LANES), V(HN // 2, keys, LANES),
        V(R, HW * LANES + HN * NOPE_N), V(R, D), V(T - 1, B, D), V(B, D, dtype=F32),
        V(Z, 2, depth, wmax), V(Z, 2, depth, wmax), V(Z, 2, wmax, ow),
        V(Z, T, B, D), V(Z, R, wmax), V(Z, R, wmax, dtype=BF if share else F32),
        V(Z, 16, wmax, dtype=F32), V(Z, 16, wmax, dtype=F32), V(R, wmax),
        V(8, LANES) if share else V(Z, T, B, D), V(Z, T - 1, B, D), V(Z + 1, B, D),
        sem(8),
        sem(Z), sem(Z), sem(Z, T), sem(Z, T), sem(Z, T), sem(Z, T), one, one,
        sem(3, Z), sem(3, Z), sem(3, Z, G), sem(3, Z, G), sem(3), sem(3), sem(3),
        sem(T, 4), sem(T, 4), sem(Z, U), sem(Z, U), sem(Z, U), sem(Z, T, U), sem(Z, T, U), one, one,
        sem(Z, T, 2), sem(Z, T, 2), sem(Z, 2), sem(Z + 1, 2),
    ]
    return pl.pallas_call(
        functools.partial(layer_kernel, n),
        out_shape=jax.ShapeDtypeStruct((B, D), BF),
        in_specs=[vmem] * 6 + [hbm] * 11,
        out_specs=vmem,
        scratch_shapes=scratch,
        compiler_params=pltpu.CompilerParams(
            collective_id=0, has_side_effects=True, vmem_limit_bytes=67043328
        ),
        name="layer",
    )(
        latent, rope_key, query_wide, query_narrow, trig, norm_gain.reshape(1, D),
        layer_input, key_up_wide, key_up_narrow, value_up_wide, value_up_narrow,
        out_wide, out_narrow, conv_weight, gate_weight, value_weight, down_weight,
    )


def solution(mesh):
    in_specs = (
        P(("grp", "sp", "tp"), None),
        P(("grp", "sp"), None),
        P(("grp", "sp"), None),
        P(("grp", "sp"), "tp"),
        P(("grp", "sp"), "tp"),
        P(None, "tp"),
        P(None, "tp"),
        P(None, "tp"),
        P(None, "tp"),
        P("tp", None),
        P("tp", None),
        P(),
        P("sp", "tp"),
        P("sp", "tp"),
        P(None, "tp"),
        P("tp", "sp"),
    )
    out_specs = P(("grp", "sp", "tp"), None)
    return jax.shard_map(
        layer, mesh=mesh, in_specs=in_specs, out_specs=out_specs, check_vma=False
    )
```

```python
import functools
import math

import jax
import jax.numpy as jnp
from jax import lax
from jax.experimental import pallas as pl
from jax.experimental.pallas import tpu as pltpu
from jax.sharding import PartitionSpec as P

NOPE_W = 128
NOPE_N = 64
LANES = 128
MESH = pl.DeviceIdType.MESH
BF = jnp.bfloat16
F32 = jnp.float32

rope_base = 10000.0
norm_eps = 1e-06


def cut_points(tiles, parts):
    plain = [k * tiles // parts for k in range(parts + 1)]
    even = [
        k * tiles // parts if 2 * k <= parts else tiles - (parts - k) * tiles // parts
        for k in range(parts + 1)
    ]

    def widest(cuts):
        return max(b - a for a, b in zip(cuts, cuts[1:]))

    return even if widest(even) <= widest(plain) else plain


def dot(a, b):
    return jnp.dot(a, b, preferred_element_type=F32)


def dot_t(a, b):
    return lax.dot_general(a, b, (((1,), (1,)), ((), ())), preferred_element_type=F32)


def layer_kernel(
    n,
    latent, rope, query_w, query_n, trig, gain,
    x_in, kuw, kun, vuw, vun, ow, on, conv, gate, value, down,
    out,
    lat, kuw_v, kun_v, vuw_v, vun_v, ow_v, xin_v,
    taps, qw, qn, kw, kn, vw, vn, att, hpb, hrecv, mid,
    wg, wv, wd, xs, gp, vp, edge, halo, hid, pb, xr, zin,
    loc,
    lzr_s, lzl_s, lz_r, lx_s, lx_r, lc_s, lc_r, lo_s, lo_r,
    wz_s, wz_r, wy_s, wy_r, wc_s, wc_r, wl,
    hx_s, hx_r, azr_s, azl_s, az_r, ax_s, ax_r, e_s, e_r,
    rx_s, rx_r, rz_s, rz_r,
):
    G, S, T = n["G"], n["S"], n["T"]
    Z = S // 2
    R = latent.shape[0]
    B = R // T
    LW = kuw.shape[0]
    D = xs.shape[3]
    HW, HN = qw.shape[0], qn.shape[0]
    WMAX = wg.shape[3]
    depth = gate.shape[0]
    cuts = cut_points(gate.shape[1] // LANES, Z)
    widths = [(b - a) * LANES for a, b in zip(cuts, cuts[1:])]
    g, s, t = lax.axis_index("grp"), lax.axis_index("sp"), lax.axis_index("tp")
    z, c = s // 2, s % 2

    def zdev(zz):
        return (g, 2 * zz + c, t)

    def xdev(tt):
        return (g, s, tt)

    sib = (g, 2 * z + 1 - c, t)
    xpart = [(t + d) % T for d in range(1, T)]
    if n["share"]:
        pb = xs

    def slot(sender, receiver):
        return (sender - receiver + T) % T - 1

    ypart = [(g + d) % G for d in range(1, G)]

    def rcopy(src, dst, ss, rs, dev):
        return pltpu.make_async_remote_copy(
            src_ref=src, dst_ref=dst, send_sem=ss, recv_sem=rs, device_id=dev, device_id_type=MESH
        )

    def got(ref, rs):
        rcopy(ref, ref, rs, rs, sib).wait_recv()

    def sent(ref, ss):
        rcopy(ref, ref, ss, ss, sib).wait_send()

    def rows(part):
        return pl.ds(pl.multiple_of(part * B, B), B)

    def by_lane(first, second, width):
        lane = lax.broadcasted_iota(jnp.int32, (R, LANES), 1)
        return jnp.where(lane < width, first, second)

    def turn(entries):
        turned = by_lane(-pltpu.roll(entries, LANES - 32, 1), pltpu.roll(entries, 32, 1), 32)
        return entries * trig[0] + turned * trig[1]

    local = [
        pltpu.make_async_copy(kuw, kuw_v, loc.at[0]),
        pltpu.make_async_copy(kun, kun_v, loc.at[1]),
        pltpu.make_async_copy(vuw, vuw_v, loc.at[2]),
        pltpu.make_async_copy(vun, vun_v, loc.at[3]),
        pltpu.make_async_copy(x_in, xin_v, loc.at[4]),
        pltpu.make_async_copy(ow, ow_v.at[pl.ds(0, HW * LANES)], loc.at[5]),
        pltpu.make_async_copy(on, ow_v.at[pl.ds(HW * LANES, HN * NOPE_N)], loc.at[6]),
    ]
    for cp in local:
        cp.start()
    lat[s, :, pl.ds(0, LW)] = latent[...]
    rot = rope.shape[0]
    wide_rows = -(-R // LANES) * LANES
    entries = jnp.concatenate([rope[...].astype(F32), jnp.zeros((LANES - rot, R), F32)], 0)
    if wide_rows > R:
        entries = jnp.concatenate([entries, jnp.zeros((LANES, wide_rows - R), F32)], 1)
    entries = entries.T[:R]
    lat[s, :, pl.ds(LW, LANES)] = turn(entries).astype(BF)

    bar = pltpu.get_barrier_semaphore()
    for zz in range(Z):
        @pl.when(zz != z)
        def _():
            pl.semaphore_signal(bar, inc=1, device_id=zdev(zz), device_id_type=MESH)
    for tt in xpart:
        pl.semaphore_signal(bar, inc=1, device_id=xdev(tt), device_id_type=MESH)
    for gg in ypart:
        pl.semaphore_signal(bar, inc=1, device_id=(gg, s, t), device_id_type=MESH)
    pl.semaphore_signal(bar, inc=1, device_id=sib, device_id_type=MESH)
    pl.semaphore_wait(bar, Z + T + G - 2)

    near = jnp.minimum(z, Z - 1 - z)
    outward = jnp.where(z < Z - 1 - z, 1, -1)

    def order(i):
        sign = jnp.where(i % 2 == 1, 1, -1)
        return jnp.where(i <= 2 * near, z + sign * ((i + 1) // 2), z + outward * (i - near))

    def pass_latents(zi):
        part = lat.at[2 * zi + c, rows(t)]

        @pl.when((zi <= z) & (z < Z - 1))
        def _():
            rcopy(part, part, lzr_s.at[zi], lz_r.at[zi], zdev(z + 1)).start()

        @pl.when((zi >= z) & (z > 0))
        def _():
            rcopy(part, part, lzl_s.at[zi], lz_r.at[zi], zdev(z - 1)).start()

    pass_latents(z)
    rcopy(lat.at[s], lat.at[s], lo_s, lo_r, sib).start()

    mats = ((gate, wg), (value, wv), (down, wd))
    hd = depth // G

    def piece(ai, zz, cc, gg, w):
        if ai < 2:
            return mats[ai][1].at[zz, cc, pl.ds(pl.multiple_of(gg * hd, hd), hd), pl.ds(0, w)]
        wh = w // G
        return wd.at[zz, cc, pl.ds(pl.multiple_of(gg * wh, wh), wh)]

    def slab(ai, cc, w):
        if ai < 2:
            return mats[ai][1].at[:, cc, :, pl.ds(0, w)]
        return wd.at[:, cc, pl.ds(0, w)]

    def own_copy(ai, zz):
        w, lo = widths[zz], cuts[zz] * LANES
        if ai < 2:
            return pltpu.make_async_copy(
                mats[ai][0].at[:, pl.ds(lo, w)], mats[ai][1].at[zz, c, :, pl.ds(0, w)], wl.at[ai]
            )
        return pltpu.make_async_copy(down.at[pl.ds(lo, w)], wd.at[zz, c, pl.ds(0, w)], wl.at[ai])

    def tap_copy(zz):
        w = widths[zz]
        return pltpu.make_async_copy(
            conv.at[:, pl.ds(cuts[zz] * LANES, w)], taps.at[:, pl.ds(0, w)], loc.at[7]
        )

    def hbm_piece(ai, zz):
        w, lo = widths[zz], cuts[zz] * LANES
        if ai < 2:
            return mats[ai][0].at[pl.ds(pl.multiple_of(g * hd, hd), hd), pl.ds(lo, w)]
        wh = w // G
        return down.at[pl.ds(pl.multiple_of(lo + g * wh, math.gcd(lo, wh) if lo else wh), wh)]

    def spread(ai):
        for zz in range(Z):
            if widths[zz]:
                @pl.when(zz != z)
                def _():
                    rcopy(
                        hbm_piece(ai, zz), piece(ai, z, c, g, widths[zz]),
                        wz_s.at[ai, zz], wz_r.at[ai, z], zdev(zz),
                    ).start()

                @pl.when(zz == z)
                def _():
                    own_copy(ai, zz).start()

    def by_width(body):
        for w in sorted(set(widths)):
            mine = functools.reduce(
                jnp.logical_or, [z == k for k in range(Z) if widths[k] == w]
            )

            @pl.when(mine)
            def _():
                body(w)

    def relay_y(ai):
        def body(w):
            if not w:
                return
            for zz in range(Z):
                @pl.when(zz != z)
                def _():
                    part = piece(ai, zz, c, g, w)
                    got(part, wz_r.at[ai, zz])
                    for gg in ypart:
                        rcopy(part, part, wy_s.at[ai, zz, gg], wy_r.at[ai, zz, g], (gg, s, t)).start()
        by_width(body)

    def relay_core(ai):
        def body(w):
            if not w:
                return
            for zz in range(Z):
                if widths[zz] == w:
                    @pl.when(zz == z)
                    def _():
                        own_copy(ai, zz).wait()
            for zz in range(Z):
                @pl.when(zz != z)
                def _():
                    for gg in ypart:
                        got(piece(ai, zz, c, gg, w), wy_r.at[ai, zz, gg])
            rcopy(slab(ai, c, w), slab(ai, c, w), wc_s.at[ai], wc_r.at[ai], sib).start()
        by_width(body)

    def arrive(ai):
        def body(w):
            if w:
                got(slab(ai, 1 - c, w), wc_r.at[ai])
        by_width(body)

    def spread_sent(ai):
        for zz in range(Z):
            if widths[zz]:
                @pl.when(zz != z)
                def _():
                    sent(hbm_piece(ai, zz), wz_s.at[ai, zz])

        def body(w):
            if not w:
                return
            for zz in range(Z):
                @pl.when(zz != z)
                def _():
                    for gg in ypart:
                        sent(piece(ai, zz, c, g, w), wy_s.at[ai, zz, gg])
            sent(slab(ai, c, w), wc_s.at[ai])
        by_width(body)


    for zz in range(Z):
        if widths[zz]:
            @pl.when(zz == z)
            def _():
                tap_copy(zz).start()

    def clear(w):
        if w < WMAX:
            gap = WMAX - w
            for ref in (wg, wv):
                ref[:, :, :, pl.ds(w, gap)] = jnp.zeros((Z, 2, depth, gap), BF)
            wd[:, :, pl.ds(w, gap), :] = jnp.zeros((Z, 2, gap, wd.shape[3]), BF)
            taps[:, pl.ds(w, gap)] = jnp.zeros((taps.shape[0], gap), F32)
    by_width(clear)

    for h in range(0, HW, 2):
        one, two, three = (
            query_w[:, pl.ds((3 * (h // 2) + i) * LANES, LANES)].astype(F32) for i in range(3)
        )
        two_r, three_r = pltpu.roll(two, 64, 1), pltpu.roll(three, 64, 1)
        qw[h, :, pl.ds(0, LANES)] = one.astype(BF)
        qw[h, :, pl.ds(LANES, LANES)] = turn(two).astype(BF)
        qw[h + 1, :, pl.ds(0, LANES)] = by_lane(two_r, three_r, 64).astype(BF)
        qw[h + 1, :, pl.ds(LANES, LANES)] = turn(three_r).astype(BF)
    for h in range(HN):
        entries = pltpu.roll(query_n[:, pl.ds(h * LANES, LANES)].astype(F32), 64, 1)
        qn[h] = by_lane(turn(entries), entries, 64).astype(BF)
    for cp in local[:4]:
        cp.wait()

    def expand(i):
        at = pl.ds(pl.multiple_of(i * R, R), R)
        low = lat[i, :, pl.ds(0, LW)]
        turned = lat[i, :, pl.ds(LW, LANES)]
        key = dot(low, kuw_v[...]).astype(BF)
        val = dot(low, vuw_v[...]).astype(BF)
        for h in range(HW):
            kw[h, at, pl.ds(0, LANES)] = key[:, h * LANES : (h + 1) * LANES]
            kw[h, at, pl.ds(LANES, LANES)] = turned
            vw[h, at, :] = val[:, h * LANES : (h + 1) * LANES]
        key = dot(low, kun_v[...]).astype(BF).astype(F32)
        val = dot(low, vun_v[...]).astype(BF)
        turned = turned.astype(F32)
        for h in range(0, HN, 2):
            pair = key[:, h * NOPE_N : h * NOPE_N + LANES]
            kn[h, at, :] = by_lane(turned, pltpu.roll(pair, 64, 1), 64).astype(BF)
            kn[h + 1, at, :] = by_lane(turned, pair, 64).astype(BF)
            vn[h // 2, at, :] = val[:, h * NOPE_N : h * NOPE_N + LANES]

    for i in range(1, Z):
        zi = order(i)
        part = lat.at[2 * zi + c, rows(t)]
        got(part, lz_r.at[zi])
        pass_latents(zi)
        for tt in xpart:
            rcopy(part, part, lx_s.at[zi, tt], lx_r.at[zi, t], xdev(tt)).start()
        rcopy(part, part, lc_s.at[zi, t], lc_r.at[zi, t], sib).start()
    spread(0)
    spread(1)
    expand(s)

    def mine(zz, carry):
        @pl.when(zz != z)
        def _():
            for tt in xpart:
                part = lat.at[2 * zz + c, rows(tt)]
                got(part, lx_r.at[zz, tt])
                rcopy(part, part, lc_s.at[zz, tt], lc_r.at[zz, tt], sib).start()
            expand(2 * zz + c)
        return carry

    lax.fori_loop(0, Z, mine, 0)
    got(lat.at[2 * z + 1 - c], lo_r)
    expand(2 * z + 1 - c)

    def theirs(zz, carry):
        @pl.when(zz != z)
        def _():
            for tt in range(T):
                got(lat.at[2 * zz + 1 - c, rows(tt)], lc_r.at[zz, tt])
            expand(2 * zz + 1 - c)
        return carry

    lax.fori_loop(0, Z, theirs, 0)

    def attend(q, k, v, scale):
        score = dot_t(q, k) * (scale * math.log2(math.e))
        prob = jnp.exp2(score - jnp.max(score, axis=-1, keepdims=True))
        total = jnp.sum(prob, axis=-1, keepdims=True)
        return dot(prob.astype(BF), v) / total

    def wide(h, carry):
        at = pl.ds(pl.multiple_of(h * LANES, LANES), LANES)
        att[:, at] = attend(qw[h], kw[h], vw[h], n["scale_w"]).astype(BF)
        return carry

    def narrow(p, carry):
        at = pl.ds(pl.multiple_of((HW + p) * LANES, LANES), LANES)
        first = attend(qn[2 * p], kn[2 * p], vn[p], n["scale_n"])
        second = attend(qn[2 * p + 1], kn[2 * p + 1], vn[p], n["scale_n"])
        att[:, at] = by_lane(first, second, 64).astype(BF)
        return carry

    lax.fori_loop(0, HW, wide, 0)
    relay_y(0)
    lax.fori_loop(0, HN // 2, narrow, 0)

    for cp in local[4:]:
        cp.wait()
    NB = n["NB"]
    cw = D // NB
    for j in range(NB):
        cols = pl.ds(j * cw, cw)
        hpb[:, cols] = dot(att[...], ow_v[:, cols]).astype(BF)
        for tt in xpart:
            rcopy(
                hpb.at[rows(tt), cols], hrecv.at[slot(t, tt), :, cols], hx_s.at[tt, j], hx_r.at[t, j], xdev(tt)
            ).start()
    for j in range(NB):
        cols = pl.ds(j * cw, cw)
        part = hpb[rows(t), cols].astype(F32)
        for tt in xpart:
            came = hrecv.at[slot(tt, t), :, cols]
            got(came, hx_r.at[tt, j])
            part = part + came[...].astype(F32)
        mid[:, cols] = (xin_v[:, cols].astype(F32) + part).astype(BF).astype(F32)
    full = mid[...]
    power = jnp.mean(full * full, axis=-1, keepdims=True)
    xs[z, t] = (full * lax.rsqrt(power + norm_eps) * gain[...]).astype(BF)

    U = n["U"]
    sub = B // U

    def strip(zi, tt, u):
        return xs.at[zi, tt, pl.ds(u * sub, sub)]

    def forward(zi, u):
        blk = strip(zi, t, u)

        @pl.when((zi <= z) & (z < Z - 1))
        def _():
            rcopy(blk, blk, azr_s.at[zi, u], az_r.at[zi, u], zdev(z + 1)).start()

        @pl.when((zi >= z) & (z > 0))
        def _():
            rcopy(blk, blk, azl_s.at[zi, u], az_r.at[zi, u], zdev(z - 1)).start()
        for tt in xpart:
            rcopy(blk, blk, ax_s.at[zi, tt, u], ax_r.at[zi, t, u], xdev(tt)).start()

    def rows_sent():
        for zz in range(Z):
            for u in range(U):
                @pl.when((zz <= z) & (z < Z - 1))
                def _():
                    sent(strip(zz, t, u), azr_s.at[zz, u])

                @pl.when((zz >= z) & (z > 0))
                def _():
                    sent(strip(zz, t, u), azl_s.at[zz, u])
                for tt in xpart:
                    sent(strip(zz, t, u), ax_s.at[zz, tt, u])

    def relay_rows(i):
        nxt = order(i)
        for u in range(U):
            got(strip(nxt, t, u), az_r.at[nxt, u])
            forward(nxt, u)

    for u in range(U):
        forward(z, u)
    relay_y(1)
    if Z > 1:
        relay_rows(1)
    spread(2)
    relay_core(0)
    arrive(0)
    relay_core(1)
    arrive(1)

    NC = WMAX // n["NW"]

    def project(i, carry):
        zi = order(i)

        for tt in xpart:
            for u in range(U):
                got(strip(zi, tt, u), ax_r.at[zi, tt, u])
        block = xs[zi].reshape(R, D)
        for j in range(n["NW"]):
            cols = pl.ds(j * NC, NC)
            pre = dot(block, wg[:, :, :, cols].reshape(D, NC)).astype(BF)
            gp[zi, :, cols] = pre
            edge[zi, pl.ds(0, 8), cols] = pre[:8].astype(F32)
            edge[zi, pl.ds(8, 8), cols] = pre[R - 8 :].astype(F32)
        for j in range(n["NW"]):
            cols = pl.ds(j * NC, NC)
            vp[zi, :, cols] = dot(block, wv[:, :, :, cols].reshape(D, NC)).astype(vp.dtype)

        @pl.when(i + 2 < Z)
        def _():
            relay_rows(i + 2)

        @pl.when(i == max(0, Z - 3))
        def _():
            relay_y(2)
        return carry

    lax.fori_loop(0, Z, project, 0)
    rcopy(edge, halo, e_s, e_r, sib).start()
    relay_core(2)
    arrive(2)
    got(halo, e_r)
    for zz in range(Z):
        if widths[zz]:
            @pl.when(zz == z)
            def _():
                tap_copy(zz).wait()
    if n["share"]:
        rows_sent()

    place = lax.broadcasted_iota(jnp.int32, (R, NC), 0)
    OW = wd.shape[3]

    J = 2
    SJ = S // J
    DJ = D // J

    def summed(zi, j):
        cols = pl.ds(j * DJ, DJ)
        total = pb[zi, t, :, cols].astype(F32)
        for tt in xpart:
            part = xr.at[zi, slot(tt, t), :, cols]
            got(part, rx_r.at[zi, tt, j])
            total = total + part[...].astype(F32)
        return total

    def add_up(zi, j):
        cols = pl.ds(j * DJ, DJ)
        total = summed(zi, j)
        inner = ((zi > z) & (z > 0)) | ((zi < z) & (z < Z - 1))
        mine = pb.at[zi, t, :, cols]

        @pl.when(inner)
        def _():
            got(zin.at[zi, :, cols], rz_r.at[zi, j])
            mine[...] = (total + zin[zi, :, cols].astype(F32)).astype(BF)

        @pl.when(jnp.logical_not(inner))
        def _():
            mine[...] = total.astype(BF)

        @pl.when(zi > z)
        def _():
            rcopy(mine, zin.at[zi, :, cols], rz_s.at[zi, j], rz_r.at[zi, j], zdev(z + 1)).start()

        @pl.when(zi < z)
        def _():
            into = jnp.where(zi == z - 1, Z, zi)
            rcopy(mine, zin.at[into, :, cols], rz_s.at[zi, j], rz_r.at[into, j], zdev(z - 1)).start()

    def mix(k, carry):
        zi = order(Z - 1 - k)
        above, below = zi - 1 + c, zi + c
        has_above = jnp.where(above >= 0, 1.0, 0.0)
        has_below = jnp.where(below < Z, 1.0, 0.0)
        above, below = jnp.maximum(above, 0), jnp.minimum(below, Z - 1)
        for j in range(n["NW"]):
            cols = pl.ds(j * NC, NC)
            pre = gp[zi, :, cols].astype(F32)
            prev = halo[above, pl.ds(8, 8), cols][7:8] * has_above
            post = halo[below, pl.ds(0, 8), cols][0:1] * has_below
            up = jnp.where(place == 0, prev, pltpu.roll(pre, 1, 0))
            dn = jnp.where(place == R - 1, post, pltpu.roll(pre, R - 1, 0))
            conv = taps[0:1, cols] * up + taps[1:2, cols] * pre + taps[2:3, cols] * dn
            hid[:, cols] = (conv / (1.0 + jnp.exp(-conv)) * vp[zi, :, cols].astype(F32)).astype(BF)
        for j in range(J):
            for b in range(j * SJ, j * SJ + SJ):
                part = dot(hid[...], wd[b // 2, b % 2]).astype(BF)
                pb[zi, :, :, pl.ds(b * OW, OW)] = part.reshape(T, B, OW)
            cols = pl.ds(j * DJ, DJ)
            for tt in xpart:
                rcopy(
                    pb.at[zi, tt, :, cols], xr.at[zi, slot(t, tt), :, cols],
                    rx_s.at[zi, tt, j], rx_r.at[zi, t, j], xdev(tt),
                ).start()
        return carry

    lax.fori_loop(0, Z, mix, 0)

    def pass_on(k, carry):
        zi = order(Z - 1 - k)
        for j in range(J):
            add_up(zi, j)
        return carry

    lax.fori_loop(0, Z - 1, pass_on, 0)
    for j in range(J):
        cols = pl.ds(j * DJ, DJ)
        mid[:, cols] = mid[:, cols] + summed(z, j)

        @pl.when(z > 0)
        def _():
            got(zin.at[z, :, cols], rz_r.at[z, j])
            mid[:, cols] = mid[:, cols] + zin[z, :, cols].astype(F32)

        @pl.when(z < Z - 1)
        def _():
            got(zin.at[Z, :, cols], rz_r.at[Z, j])
            mid[:, cols] = mid[:, cols] + zin[Z, :, cols].astype(F32)
    out[...] = mid[...]

    sent(lat.at[s], lo_s)
    sent(edge, e_s)
    for ai in range(3):
        spread_sent(ai)
    for tt in xpart:
        for j in range(NB):
            sent(hpb.at[rows(tt), pl.ds(j * cw, cw)], hx_s.at[tt, j])
    for zz in range(Z):
        part = lat.at[2 * zz + c, rows(t)]

        @pl.when((zz <= z) & (z < Z - 1))
        def _():
            sent(part, lzr_s.at[zz])

        @pl.when((zz >= z) & (z > 0))
        def _():
            sent(part, lzl_s.at[zz])

        @pl.when(zz != z)
        def _():
            for tt in xpart:
                sent(part, lx_s.at[zz, tt])
            for tt in range(T):
                sent(part, lc_s.at[zz, tt])
            for j in range(J):
                sent(pb.at[zz, t, :, pl.ds(j * DJ, DJ)], rz_s.at[zz, j])
        for tt in xpart:
            for j in range(J):
                sent(pb.at[zz, tt, :, pl.ds(j * DJ, DJ)], rx_s.at[zz, tt, j])
    if not n["share"]:
        rows_sent()


def rope_tables(row_start, row_total, span_width):
    places = (row_start + jnp.arange(row_total, dtype=jnp.int32)).astype(F32)
    frequency = jnp.power(
        rope_base, -jnp.arange(0, span_width, 2, dtype=jnp.int32).astype(F32) / span_width
    )
    angles = places[:, None] * jnp.tile(frequency, 2 * LANES // span_width)[None, :]
    valid = jnp.arange(LANES) < span_width
    return jnp.where(valid, jnp.stack([jnp.cos(angles), jnp.sin(angles)]), 0.0)


def layer(
    layer_input,
    latent,
    rope_key,
    query_wide,
    query_narrow,
    key_up_wide,
    value_up_wide,
    key_up_narrow,
    value_up_narrow,
    out_wide,
    out_narrow,
    norm_gain,
    gate_weight,
    value_weight,
    conv_weight,
    down_weight,
):
    G, S, T = lax.axis_size("grp"), lax.axis_size("sp"), lax.axis_size("tp")
    Z = S // 2
    R, LW = latent.shape
    rot = rope_key.shape[1]
    D = layer_input.shape[1]
    B = R // T
    HW = key_up_wide.shape[1] // NOPE_W
    HN = key_up_narrow.shape[1] // NOPE_N
    trig = rope_tables(lax.axis_index("sp") * R, R, rot)
    tiles = gate_weight.shape[1] // LANES
    cuts = cut_points(tiles, Z)
    wmax = max(b - a for a, b in zip(cuts, cuts[1:])) * LANES
    keys = S * R
    depth, ow = gate_weight.shape[0], down_weight.shape[1]
    U = 2 if B % 32 == 0 else 1
    share = Z * T * B * D * 2 > 8 << 20
    n = dict(
        share=share,
        U=U,
        G=G,
        S=S,
        T=T,
        NB=4,
        NW=max(1, wmax // 256),
        scale_w=1.0 / math.sqrt(NOPE_W + rot),
        scale_n=1.0 / math.sqrt(NOPE_N + rot),
    )
    vmem = pl.BlockSpec(memory_space=pltpu.VMEM)
    hbm = pl.BlockSpec(memory_space=pl.ANY)

    def V(*shape, dtype=BF):
        return pltpu.VMEM(shape, dtype)

    def sem(*shape):
        return pltpu.SemaphoreType.DMA(shape)

    one = pltpu.SemaphoreType.DMA
    scratch = [
        V(S, R, LW + LANES),
        V(*key_up_wide.shape), V(*key_up_narrow.shape),
        V(*value_up_wide.shape), V(*value_up_narrow.shape),
        V(HW * LANES + HN * NOPE_N, D), V(B, D), V(conv_weight.shape[0], wmax, dtype=F32),
        V(HW, R, 2 * LANES), V(HN, R, LANES),
        V(HW, keys, 2 * LANES), V(HN, keys, LANES), V(HW, keys, LANES), V(HN // 2, keys, LANES),
        V(R, HW * LANES + HN * NOPE_N), V(R, D), V(T - 1, B, D), V(B, D, dtype=F32),
        V(Z, 2, depth, wmax), V(Z, 2, depth, wmax), V(Z, 2, wmax, ow),
        V(Z, T, B, D), V(Z, R, wmax), V(Z, R, wmax, dtype=BF if share else F32),
        V(Z, 16, wmax, dtype=F32), V(Z, 16, wmax, dtype=F32), V(R, wmax),
        V(8, LANES) if share else V(Z, T, B, D), V(Z, T - 1, B, D), V(Z + 1, B, D),
        sem(8),
        sem(Z), sem(Z), sem(Z), sem(Z, T), sem(Z, T), sem(Z, T), sem(Z, T), one, one,
        sem(3, Z), sem(3, Z), sem(3, Z, G), sem(3, Z, G), sem(3), sem(3), sem(3),
        sem(T, 4), sem(T, 4), sem(Z, U), sem(Z, U), sem(Z, U), sem(Z, T, U), sem(Z, T, U), one, one,
        sem(Z, T, 2), sem(Z, T, 2), sem(Z, 2), sem(Z + 1, 2),
    ]
    return pl.pallas_call(
        functools.partial(layer_kernel, n),
        out_shape=jax.ShapeDtypeStruct((B, D), F32),
        in_specs=[vmem] * 6 + [hbm] * 11,
        out_specs=vmem,
        scratch_shapes=scratch,
        compiler_params=pltpu.CompilerParams(
            collective_id=0, has_side_effects=True, vmem_limit_bytes=67043328
        ),
        name="layer",
    )(
        latent, rope_key.T, query_wide, query_narrow, trig, norm_gain.reshape(1, D),
        layer_input, key_up_wide, key_up_narrow, value_up_wide, value_up_narrow,
        out_wide, out_narrow, conv_weight, gate_weight, value_weight, down_weight,
    ).astype(BF)


def solution(mesh):
    in_specs = (
        P(("grp", "sp", "tp"), None),
        P(("grp", "sp"), None),
        P(("grp", "sp"), None),
        P(("grp", "sp"), "tp"),
        P(("grp", "sp"), "tp"),
        P(None, "tp"),
        P(None, "tp"),
        P(None, "tp"),
        P(None, "tp"),
        P("tp", None),
        P("tp", None),
        P(),
        P("sp", "tp"),
        P("sp", "tp"),
        P(None, "tp"),
        P("tp", "sp"),
    )
    out_specs = P(("grp", "sp", "tp"), None)
    return jax.shard_map(
        layer, mesh=mesh, in_specs=in_specs, out_specs=out_specs, check_vma=False
    )
```

```python
import functools
import math

import jax
import jax.numpy as jnp
from jax import lax
from jax.experimental import pallas as pl
from jax.experimental.pallas import tpu as pltpu
from jax.sharding import PartitionSpec as P

NOPE_W = 128
NOPE_N = 64
LANES = 128
MESH = pl.DeviceIdType.MESH
BF = jnp.bfloat16
F32 = jnp.float32

rope_base = 10000.0
norm_eps = 1e-06


def cut_points(tiles, parts):
    plain = [k * tiles // parts for k in range(parts + 1)]
    even = [
        k * tiles // parts if 2 * k <= parts else tiles - (parts - k) * tiles // parts
        for k in range(parts + 1)
    ]

    def widest(cuts):
        return max(b - a for a, b in zip(cuts, cuts[1:]))

    return even if widest(even) <= widest(plain) else plain


def dot(a, b):
    return jnp.dot(a, b, preferred_element_type=F32)


def dot_t(a, b):
    return lax.dot_general(a, b, (((1,), (1,)), ((), ())), preferred_element_type=F32)


def layer_kernel(
    n,
    latent, rope, query_w, query_n, trig, gain,
    x_in, kuw, kun, vuw, vun, ow, on, conv, gate, value, down,
    out,
    lat, kuw_v, kun_v, vuw_v, vun_v, ow_v, xin_v,
    taps, qw, qn, kw, kn, vw, vn, att, hpb, hrecv, mid,
    wg, wv, wd, xs, gp, vp, edge, halo, hid, pb, xr, zin, acc, beside_in,
    loc,
    lzr_s, lzl_s, lz_r, lx_s, lx_r, lc_s, lc_r, lo_s, lo_r,
    wz_s, wz_r, wy_s, wy_r, wc_s, wc_r, wl,
    hx_s, hx_r, azr_s, azl_s, az_r, ax_s, ax_r, e_s, e_r,
    rx_s, rx_r, rz_s, rz_r, nb_s, nb_r,
):
    G, S, T = n["G"], n["S"], n["T"]
    Z = S // 2
    R = latent.shape[0]
    B = R // T
    LW = kuw.shape[0]
    D = xs.shape[3]
    HW, HN = qw.shape[0], qn.shape[0]
    WMAX = wg.shape[3]
    depth = gate.shape[0]
    cuts = cut_points(gate.shape[1] // LANES, Z)
    widths = [(b - a) * LANES for a, b in zip(cuts, cuts[1:])]
    g, s, t = lax.axis_index("grp"), lax.axis_index("sp"), lax.axis_index("tp")
    z, c = s // 2, s % 2

    def zdev(zz):
        return (g, 2 * zz + c, t)

    def xdev(tt):
        return (g, s, tt)

    sib = (g, 2 * z + 1 - c, t)
    xpart = [(t + d) % T for d in range(1, T)]
    if n["share"]:
        pb = xs

    def slot(sender, receiver):
        return (sender - receiver + T) % T - 1

    ypart = [(g + d) % G for d in range(1, G)]

    def rcopy(src, dst, ss, rs, dev):
        return pltpu.make_async_remote_copy(
            src_ref=src, dst_ref=dst, send_sem=ss, recv_sem=rs, device_id=dev, device_id_type=MESH
        )

    def got(ref, rs):
        rcopy(ref, ref, rs, rs, sib).wait_recv()

    def sent(ref, ss):
        rcopy(ref, ref, ss, ss, sib).wait_send()

    def rows(part):
        return pl.ds(pl.multiple_of(part * B, B), B)

    def by_lane(first, second, width):
        lane = lax.broadcasted_iota(jnp.int32, (R, LANES), 1)
        return jnp.where(lane < width, first, second)

    def turn(entries):
        turned = by_lane(-pltpu.roll(entries, LANES - 32, 1), pltpu.roll(entries, 32, 1), 32)
        return entries * trig[0] + turned * trig[1]

    local = [
        pltpu.make_async_copy(kuw, kuw_v, loc.at[0]),
        pltpu.make_async_copy(kun, kun_v, loc.at[1]),
        pltpu.make_async_copy(vuw, vuw_v, loc.at[2]),
        pltpu.make_async_copy(vun, vun_v, loc.at[3]),
        pltpu.make_async_copy(x_in, xin_v, loc.at[4]),
        pltpu.make_async_copy(ow, ow_v.at[pl.ds(0, HW * LANES)], loc.at[5]),
        pltpu.make_async_copy(on, ow_v.at[pl.ds(HW * LANES, HN * NOPE_N)], loc.at[6]),
    ]
    for cp in local:
        cp.start()
    lat[s, :, pl.ds(0, LW)] = latent[...]
    rot = rope.shape[0]
    wide_rows = -(-R // LANES) * LANES
    entries = jnp.concatenate([rope[...].astype(F32), jnp.zeros((LANES - rot, R), F32)], 0)
    if wide_rows > R:
        entries = jnp.concatenate([entries, jnp.zeros((LANES, wide_rows - R), F32)], 1)
    entries = entries.T[:R]
    lat[s, :, pl.ds(LW, LANES)] = turn(entries).astype(BF)

    bar = pltpu.get_barrier_semaphore()
    for zz in range(Z):
        @pl.when(zz != z)
        def _():
            pl.semaphore_signal(bar, inc=1, device_id=zdev(zz), device_id_type=MESH)
    for tt in xpart:
        pl.semaphore_signal(bar, inc=1, device_id=xdev(tt), device_id_type=MESH)
    for gg in ypart:
        pl.semaphore_signal(bar, inc=1, device_id=(gg, s, t), device_id_type=MESH)
    pl.semaphore_signal(bar, inc=1, device_id=sib, device_id_type=MESH)
    pl.semaphore_wait(bar, Z + T + G - 2)

    near = jnp.minimum(z, Z - 1 - z)
    outward = jnp.where(z < Z - 1 - z, 1, -1)

    def order(i):
        sign = jnp.where(i % 2 == 1, 1, -1)
        return jnp.where(i <= 2 * near, z + sign * ((i + 1) // 2), z + outward * (i - near))

    def pass_latents(zi):
        part = lat.at[2 * zi + c, rows(t)]

        @pl.when((zi <= z) & (z < Z - 1))
        def _():
            rcopy(part, part, lzr_s.at[zi], lz_r.at[zi], zdev(z + 1)).start()

        @pl.when((zi >= z) & (z > 0))
        def _():
            rcopy(part, part, lzl_s.at[zi], lz_r.at[zi], zdev(z - 1)).start()

    pass_latents(z)
    rcopy(lat.at[s], lat.at[s], lo_s, lo_r, sib).start()

    mats = ((gate, wg), (value, wv), (down, wd))
    hd = depth // G

    def piece(ai, zz, cc, gg, w):
        if ai < 2:
            return mats[ai][1].at[zz, cc, pl.ds(pl.multiple_of(gg * hd, hd), hd), pl.ds(0, w)]
        wh = w // G
        return wd.at[zz, cc, pl.ds(pl.multiple_of(gg * wh, wh), wh)]

    def slab(ai, cc, w):
        if ai < 2:
            return mats[ai][1].at[:, cc, :, pl.ds(0, w)]
        return wd.at[:, cc, pl.ds(0, w)]

    def own_copy(ai, zz):
        w, lo = widths[zz], cuts[zz] * LANES
        if ai < 2:
            return pltpu.make_async_copy(
                mats[ai][0].at[:, pl.ds(lo, w)], mats[ai][1].at[zz, c, :, pl.ds(0, w)], wl.at[ai]
            )
        return pltpu.make_async_copy(down.at[pl.ds(lo, w)], wd.at[zz, c, pl.ds(0, w)], wl.at[ai])

    def tap_copy(zz):
        w = widths[zz]
        return pltpu.make_async_copy(
            conv.at[:, pl.ds(cuts[zz] * LANES, w)], taps.at[:, pl.ds(0, w)], loc.at[7]
        )

    def hbm_piece(ai, zz):
        w, lo = widths[zz], cuts[zz] * LANES
        if ai < 2:
            return mats[ai][0].at[pl.ds(pl.multiple_of(g * hd, hd), hd), pl.ds(lo, w)]
        wh = w // G
        return down.at[pl.ds(pl.multiple_of(lo + g * wh, math.gcd(lo, wh) if lo else wh), wh)]

    def spread(ai):
        for zz in range(Z):
            if widths[zz]:
                @pl.when(zz != z)
                def _():
                    rcopy(
                        hbm_piece(ai, zz), piece(ai, z, c, g, widths[zz]),
                        wz_s.at[ai, zz], wz_r.at[ai, z], zdev(zz),
                    ).start()

                @pl.when(zz == z)
                def _():
                    own_copy(ai, zz).start()

    def by_width(body):
        for w in sorted(set(widths)):
            mine = functools.reduce(
                jnp.logical_or, [z == k for k in range(Z) if widths[k] == w]
            )

            @pl.when(mine)
            def _():
                body(w)

    def relay_y(ai):
        def body(w):
            if not w:
                return
            for zz in range(Z):
                @pl.when(zz != z)
                def _():
                    part = piece(ai, zz, c, g, w)
                    got(part, wz_r.at[ai, zz])
                    for gg in ypart:
                        rcopy(part, part, wy_s.at[ai, zz, gg], wy_r.at[ai, zz, g], (gg, s, t)).start()
        by_width(body)

    def relay_core(ai):
        def body(w):
            if not w:
                return
            for zz in range(Z):
                if widths[zz] == w:
                    @pl.when(zz == z)
                    def _():
                        own_copy(ai, zz).wait()
            for zz in range(Z):
                @pl.when(zz != z)
                def _():
                    for gg in ypart:
                        got(piece(ai, zz, c, gg, w), wy_r.at[ai, zz, gg])
            rcopy(slab(ai, c, w), slab(ai, c, w), wc_s.at[ai], wc_r.at[ai], sib).start()
        by_width(body)

    def arrive(ai):
        def body(w):
            if w:
                got(slab(ai, 1 - c, w), wc_r.at[ai])
        by_width(body)

    def spread_sent(ai):
        for zz in range(Z):
            if widths[zz]:
                @pl.when(zz != z)
                def _():
                    sent(hbm_piece(ai, zz), wz_s.at[ai, zz])

        def body(w):
            if not w:
                return
            for zz in range(Z):
                @pl.when(zz != z)
                def _():
                    for gg in ypart:
                        sent(piece(ai, zz, c, g, w), wy_s.at[ai, zz, gg])
            sent(slab(ai, c, w), wc_s.at[ai])
        by_width(body)


    for zz in range(Z):
        if widths[zz]:
            @pl.when(zz == z)
            def _():
                tap_copy(zz).start()

    def clear(w):
        if w < WMAX:
            gap = WMAX - w
            for ref in (wg, wv):
                ref[:, :, :, pl.ds(w, gap)] = jnp.zeros((Z, 2, depth, gap), BF)
            wd[:, :, pl.ds(w, gap), :] = jnp.zeros((Z, 2, gap, wd.shape[3]), BF)
            taps[:, pl.ds(w, gap)] = jnp.zeros((taps.shape[0], gap), F32)
    by_width(clear)

    for h in range(0, HW, 2):
        one, two, three = (
            query_w[:, pl.ds((3 * (h // 2) + i) * LANES, LANES)].astype(F32) for i in range(3)
        )
        two_r, three_r = pltpu.roll(two, 64, 1), pltpu.roll(three, 64, 1)
        qw[h, :, pl.ds(0, LANES)] = one.astype(BF)
        qw[h, :, pl.ds(LANES, LANES)] = turn(two).astype(BF)
        qw[h + 1, :, pl.ds(0, LANES)] = by_lane(two_r, three_r, 64).astype(BF)
        qw[h + 1, :, pl.ds(LANES, LANES)] = turn(three_r).astype(BF)
    for h in range(HN):
        entries = pltpu.roll(query_n[:, pl.ds(h * LANES, LANES)].astype(F32), 64, 1)
        qn[h] = by_lane(turn(entries), entries, 64).astype(BF)
    for cp in local[:4]:
        cp.wait()

    def expand(i):
        at = pl.ds(pl.multiple_of(i * R, R), R)
        low = lat[i, :, pl.ds(0, LW)]
        turned = lat[i, :, pl.ds(LW, LANES)]
        key = dot(low, kuw_v[...]).astype(BF)
        val = dot(low, vuw_v[...]).astype(BF)
        for h in range(HW):
            kw[h, at, pl.ds(0, LANES)] = key[:, h * LANES : (h + 1) * LANES]
            kw[h, at, pl.ds(LANES, LANES)] = turned
            vw[h, at, :] = val[:, h * LANES : (h + 1) * LANES]
        key = dot(low, kun_v[...]).astype(BF).astype(F32)
        val = dot(low, vun_v[...]).astype(BF)
        turned = turned.astype(F32)
        for h in range(0, HN, 2):
            pair = key[:, h * NOPE_N : h * NOPE_N + LANES]
            kn[h, at, :] = by_lane(turned, pltpu.roll(pair, 64, 1), 64).astype(BF)
            kn[h + 1, at, :] = by_lane(turned, pair, 64).astype(BF)
            vn[h // 2, at, :] = val[:, h * NOPE_N : h * NOPE_N + LANES]

    for i in range(1, Z):
        zi = order(i)
        part = lat.at[2 * zi + c, rows(t)]
        got(part, lz_r.at[zi])
        pass_latents(zi)
        for tt in xpart:
            rcopy(part, part, lx_s.at[zi, tt], lx_r.at[zi, t], xdev(tt)).start()
        rcopy(part, part, lc_s.at[zi, t], lc_r.at[zi, t], sib).start()
    spread(0)
    spread(1)
    expand(s)

    def mine(zz, carry):
        @pl.when(zz != z)
        def _():
            for tt in xpart:
                part = lat.at[2 * zz + c, rows(tt)]
                got(part, lx_r.at[zz, tt])
                rcopy(part, part, lc_s.at[zz, tt], lc_r.at[zz, tt], sib).start()
            expand(2 * zz + c)
        return carry

    lax.fori_loop(0, Z, mine, 0)
    got(lat.at[2 * z + 1 - c], lo_r)
    expand(2 * z + 1 - c)

    def theirs(zz, carry):
        @pl.when(zz != z)
        def _():
            for tt in range(T):
                got(lat.at[2 * zz + 1 - c, rows(tt)], lc_r.at[zz, tt])
            expand(2 * zz + 1 - c)
        return carry

    lax.fori_loop(0, Z, theirs, 0)

    def attend(q, k, v, scale):
        score = dot_t(q, k) * (scale * math.log2(math.e))
        prob = jnp.exp2(score - jnp.max(score, axis=-1, keepdims=True))
        total = jnp.sum(prob, axis=-1, keepdims=True)
        return dot(prob.astype(BF), v) / total

    def wide(h, carry):
        at = pl.ds(pl.multiple_of(h * LANES, LANES), LANES)
        att[:, at] = attend(qw[h], kw[h], vw[h], n["scale_w"]).astype(BF)
        return carry

    def narrow(p, carry):
        at = pl.ds(pl.multiple_of((HW + p) * LANES, LANES), LANES)
        first = attend(qn[2 * p], kn[2 * p], vn[p], n["scale_n"])
        second = attend(qn[2 * p + 1], kn[2 * p + 1], vn[p], n["scale_n"])
        att[:, at] = by_lane(first, second, 64).astype(BF)
        return carry

    lax.fori_loop(0, HW, wide, 0)
    relay_y(0)
    lax.fori_loop(0, HN // 2, narrow, 0)

    for cp in local[4:]:
        cp.wait()
    NB = n["NB"]
    cw = D // NB
    for j in range(NB):
        cols = pl.ds(j * cw, cw)
        hpb[:, cols] = dot(att[...], ow_v[:, cols]).astype(BF)
        for tt in xpart:
            rcopy(
                hpb.at[rows(tt), cols], hrecv.at[slot(t, tt), :, cols], hx_s.at[tt, j], hx_r.at[t, j], xdev(tt)
            ).start()
    for j in range(NB):
        cols = pl.ds(j * cw, cw)
        part = hpb[rows(t), cols].astype(F32)
        for tt in xpart:
            came = hrecv.at[slot(tt, t), :, cols]
            got(came, hx_r.at[tt, j])
            part = part + came[...].astype(F32)
        mid[:, cols] = (xin_v[:, cols].astype(F32) + part).astype(BF).astype(F32)
    full = mid[...]
    power = jnp.mean(full * full, axis=-1, keepdims=True)
    xs[z, t] = (full * lax.rsqrt(power + norm_eps) * gain[...]).astype(BF)

    U = n["U"]
    sub = B // U

    def strip(zi, tt, u):
        return xs.at[zi, tt, pl.ds(u * sub, sub)]

    def forward(zi, u):
        blk = strip(zi, t, u)

        @pl.when((zi <= z) & (z < Z - 1))
        def _():
            rcopy(blk, blk, azr_s.at[zi, u], az_r.at[zi, u], zdev(z + 1)).start()

        @pl.when((zi >= z) & (z > 0))
        def _():
            rcopy(blk, blk, azl_s.at[zi, u], az_r.at[zi, u], zdev(z - 1)).start()
        for tt in xpart:
            rcopy(blk, blk, ax_s.at[zi, tt, u], ax_r.at[zi, t, u], xdev(tt)).start()

    def rows_sent():
        for zz in range(Z):
            for u in range(U):
                @pl.when((zz <= z) & (z < Z - 1))
                def _():
                    sent(strip(zz, t, u), azr_s.at[zz, u])

                @pl.when((zz >= z) & (z > 0))
                def _():
                    sent(strip(zz, t, u), azl_s.at[zz, u])
                for tt in xpart:
                    sent(strip(zz, t, u), ax_s.at[zz, tt, u])

    def relay_rows(i):
        nxt = order(i)
        for u in range(U):
            got(strip(nxt, t, u), az_r.at[nxt, u])
            forward(nxt, u)

    for u in range(U):
        forward(z, u)
    relay_y(1)
    relay_core(0)
    if Z > 1:
        relay_rows(1)
    spread(2)
    arrive(0)
    relay_core(1)
    arrive(1)

    NC = WMAX // n["NW"]

    def project(i, carry):
        zi = order(i)

        for tt in xpart:
            for u in range(U):
                got(strip(zi, tt, u), ax_r.at[zi, tt, u])
        block = xs[zi].reshape(R, D)
        for j in range(n["NW"]):
            cols = pl.ds(j * NC, NC)
            pre = dot(block, wg[:, :, :, cols].reshape(D, NC)).astype(BF)
            gp[zi, :, cols] = pre
            edge[zi, pl.ds(0, 8), cols] = pre[:8].astype(F32)
            edge[zi, pl.ds(8, 8), cols] = pre[R - 8 :].astype(F32)
        for j in range(n["NW"]):
            cols = pl.ds(j * NC, NC)
            vp[zi, :, cols] = dot(block, wv[:, :, :, cols].reshape(D, NC)).astype(vp.dtype)

        @pl.when(i + 2 < Z)
        def _():
            relay_rows(i + 2)

        @pl.when(i == max(0, Z - 4))
        def _():
            relay_y(2)
        return carry

    lax.fori_loop(0, Z, project, 0)
    rcopy(edge, halo, e_s, e_r, sib).start()
    relay_core(2)
    arrive(2)
    got(halo, e_r)
    for zz in range(Z):
        if widths[zz]:
            @pl.when(zz == z)
            def _():
                tap_copy(zz).wait()
    if n["share"]:
        rows_sent()

    place = lax.broadcasted_iota(jnp.int32, (R, NC), 0)
    OW = wd.shape[3]

    J = 2
    SJ = S // J
    DJ = D // J

    last = pl.ds((J - 1) * DJ, DJ)

    def beside(zi):
        return (zi == z - 1) | (zi == z + 1)

    def cross(zi, j):
        cols = pl.ds(j * DJ, DJ)
        for tt in xpart:
            rcopy(
                pb.at[zi, tt, :, cols], xr.at[zi, slot(t, tt), :, cols],
                rx_s.at[zi, tt, j], rx_r.at[zi, t, j], xdev(tt),
            ).start()

    def own_rows():
        for tt in xpart:
            for side, there in ((0, z > 0), (1, z < Z - 1)):
                @pl.when(there)
                def _():
                    part = beside_in.at[side, slot(tt, t)]
                    got(part, nb_r.at[side, tt])
                    pb[z, tt, :, last] = (
                        pb[z, tt, :, last].astype(F32) + part[...].astype(F32)
                    ).astype(BF)
        cross(z, J - 1)

    def summed(zi, j, own=False):
        cols = pl.ds(j * DJ, DJ)
        total = pb[zi, t, :, cols].astype(F32)
        if n["near"] and j == J - 1 and not own:
            acc[...] = total

            @pl.when(jnp.logical_not(beside(zi)))
            def _():
                for tt in xpart:
                    part = xr.at[zi, slot(tt, t), :, cols]
                    got(part, rx_r.at[zi, tt, j])
                    acc[...] = acc[...] + part[...].astype(F32)
            return acc[...]
        for tt in xpart:
            part = xr.at[zi, slot(tt, t), :, cols]
            got(part, rx_r.at[zi, tt, j])
            total = total + part[...].astype(F32)
        return total

    def add_up(zi, j):
        cols = pl.ds(j * DJ, DJ)
        total = summed(zi, j)
        inner = ((zi > z) & (z > 0)) | ((zi < z) & (z < Z - 1))
        mine = pb.at[zi, t, :, cols]

        @pl.when(inner)
        def _():
            got(zin.at[zi, :, cols], rz_r.at[zi, j])
            mine[...] = (total + zin[zi, :, cols].astype(F32)).astype(BF)

        @pl.when(jnp.logical_not(inner))
        def _():
            mine[...] = total.astype(BF)

        @pl.when(zi > z)
        def _():
            rcopy(mine, zin.at[zi, :, cols], rz_s.at[zi, j], rz_r.at[zi, j], zdev(z + 1)).start()

        @pl.when(zi < z)
        def _():
            into = jnp.where(zi == z - 1, Z, zi)
            rcopy(mine, zin.at[into, :, cols], rz_s.at[zi, j], rz_r.at[into, j], zdev(z - 1)).start()

    def mix(k, carry):
        zi = order(Z - 1 - k)
        above, below = zi - 1 + c, zi + c
        has_above = jnp.where(above >= 0, 1.0, 0.0)
        has_below = jnp.where(below < Z, 1.0, 0.0)
        above, below = jnp.maximum(above, 0), jnp.minimum(below, Z - 1)
        for j in range(n["NW"]):
            cols = pl.ds(j * NC, NC)
            pre = gp[zi, :, cols].astype(F32)
            prev = halo[above, pl.ds(8, 8), cols][7:8] * has_above
            post = halo[below, pl.ds(0, 8), cols][0:1] * has_below
            up = jnp.where(place == 0, prev, pltpu.roll(pre, 1, 0))
            dn = jnp.where(place == R - 1, post, pltpu.roll(pre, R - 1, 0))
            conv = taps[0:1, cols] * up + taps[1:2, cols] * pre + taps[2:3, cols] * dn
            hid[:, cols] = (conv / (1.0 + jnp.exp(-conv)) * vp[zi, :, cols].astype(F32)).astype(BF)
        for j in range(J):
            for b in range(j * SJ, j * SJ + SJ):
                part = dot(hid[...], wd[b // 2, b % 2]).astype(BF)
                pb[zi, :, :, pl.ds(b * OW, OW)] = part.reshape(T, B, OW)
            if n["near"] and j == J - 1:
                @pl.when(jnp.logical_not(beside(zi)) & (zi != z))
                def _():
                    cross(zi, j)

                @pl.when(beside(zi))
                def _():
                    side = jnp.where(zi < z, 1, 0)
                    for tt in xpart:
                        rcopy(
                            pb.at[zi, tt, :, last], beside_in.at[side, slot(tt, t)],
                            nb_s.at[side, tt], nb_r.at[side, tt], zdev(zi),
                        ).start()
            else:
                cross(zi, j)
        return carry

    lax.fori_loop(0, Z, mix, 0)

    def pass_on(k, carry):
        zi = order(Z - 1 - k)
        if n["near"]:
            @pl.when(k == 1)
            def _():
                own_rows()
        for j in range(J):
            add_up(zi, j)
        return carry

    lax.fori_loop(0, Z - 1, pass_on, 0)
    for j in range(J):
        cols = pl.ds(j * DJ, DJ)
        mid[:, cols] = mid[:, cols] + summed(z, j, own=True)

        @pl.when(z > 0)
        def _():
            got(zin.at[z, :, cols], rz_r.at[z, j])
            mid[:, cols] = mid[:, cols] + zin[z, :, cols].astype(F32)

        @pl.when(z < Z - 1)
        def _():
            got(zin.at[Z, :, cols], rz_r.at[Z, j])
            mid[:, cols] = mid[:, cols] + zin[Z, :, cols].astype(F32)
    out[...] = mid[...]

    sent(lat.at[s], lo_s)
    sent(edge, e_s)
    for ai in range(3):
        spread_sent(ai)
    for tt in xpart:
        for j in range(NB):
            sent(hpb.at[rows(tt), pl.ds(j * cw, cw)], hx_s.at[tt, j])
    for zz in range(Z):
        part = lat.at[2 * zz + c, rows(t)]

        @pl.when((zz <= z) & (z < Z - 1))
        def _():
            sent(part, lzr_s.at[zz])

        @pl.when((zz >= z) & (z > 0))
        def _():
            sent(part, lzl_s.at[zz])

        @pl.when(zz != z)
        def _():
            for tt in xpart:
                sent(part, lx_s.at[zz, tt])
            for tt in range(T):
                sent(part, lc_s.at[zz, tt])
            for j in range(J):
                sent(pb.at[zz, t, :, pl.ds(j * DJ, DJ)], rz_s.at[zz, j])
        for tt in xpart:
            for j in range(J):
                if n["near"] and j == J - 1:
                    @pl.when(jnp.logical_not(beside(zz)))
                    def _():
                        sent(pb.at[zz, tt, :, last], rx_s.at[zz, tt, j])
                else:
                    sent(pb.at[zz, tt, :, pl.ds(j * DJ, DJ)], rx_s.at[zz, tt, j])
    if n["near"]:
        for side, there in ((0, z < Z - 1), (1, z > 0)):
            @pl.when(there)
            def _():
                for tt in xpart:
                    sent(pb.at[z, tt, :, last], nb_s.at[side, tt])
    if not n["share"]:
        rows_sent()


def rope_tables(row_start, row_total, span_width):
    places = (row_start + jnp.arange(row_total, dtype=jnp.int32)).astype(F32)
    frequency = jnp.power(
        rope_base, -jnp.arange(0, span_width, 2, dtype=jnp.int32).astype(F32) / span_width
    )
    angles = places[:, None] * jnp.tile(frequency, 2 * LANES // span_width)[None, :]
    valid = jnp.arange(LANES) < span_width
    return jnp.where(valid, jnp.stack([jnp.cos(angles), jnp.sin(angles)]), 0.0)


def layer(
    layer_input,
    latent,
    rope_key,
    query_wide,
    query_narrow,
    key_up_wide,
    value_up_wide,
    key_up_narrow,
    value_up_narrow,
    out_wide,
    out_narrow,
    norm_gain,
    gate_weight,
    value_weight,
    conv_weight,
    down_weight,
):
    G, S, T = lax.axis_size("grp"), lax.axis_size("sp"), lax.axis_size("tp")
    Z = S // 2
    R, LW = latent.shape
    rot = rope_key.shape[1]
    D = layer_input.shape[1]
    B = R // T
    HW = key_up_wide.shape[1] // NOPE_W
    HN = key_up_narrow.shape[1] // NOPE_N
    trig = rope_tables(lax.axis_index("sp") * R, R, rot)
    tiles = gate_weight.shape[1] // LANES
    cuts = cut_points(tiles, Z)
    wmax = max(b - a for a, b in zip(cuts, cuts[1:])) * LANES
    keys = S * R
    depth, ow = gate_weight.shape[0], down_weight.shape[1]
    U = 2 if B % 32 == 0 else 1
    share = Z * T * B * D * 2 > 8 << 20
    near = not share and Z > 2
    small = (B, D // 2) if near else (8, LANES)
    n = dict(
        share=share,
        near=near,
        U=U,
        G=G,
        S=S,
        T=T,
        NB=4,
        NW=max(1, wmax // 256),
        scale_w=1.0 / math.sqrt(NOPE_W + rot),
        scale_n=1.0 / math.sqrt(NOPE_N + rot),
    )
    vmem = pl.BlockSpec(memory_space=pltpu.VMEM)
    hbm = pl.BlockSpec(memory_space=pl.ANY)

    def V(*shape, dtype=BF):
        return pltpu.VMEM(shape, dtype)

    def sem(*shape):
        return pltpu.SemaphoreType.DMA(shape)

    one = pltpu.SemaphoreType.DMA
    scratch = [
        V(S, R, LW + LANES),
        V(*key_up_wide.shape), V(*key_up_narrow.shape),
        V(*value_up_wide.shape), V(*value_up_narrow.shape),
        V(HW * LANES + HN * NOPE_N, D), V(B, D), V(conv_weight.shape[0], wmax, dtype=F32),
        V(HW, R, 2 * LANES), V(HN, R, LANES),
        V(HW, keys, 2 * LANES), V(HN, keys, LANES), V(HW, keys, LANES), V(HN // 2, keys, LANES),
        V(R, HW * LANES + HN * NOPE_N), V(R, D), V(T - 1, B, D), V(B, D, dtype=F32),
        V(Z, 2, depth, wmax), V(Z, 2, depth, wmax), V(Z, 2, wmax, ow),
        V(Z, T, B, D), V(Z, R, wmax), V(Z, R, wmax, dtype=BF if share else F32),
        V(Z, 16, wmax, dtype=F32), V(Z, 16, wmax, dtype=F32), V(R, wmax),
        V(8, LANES) if share else V(Z, T, B, D), V(Z, T - 1, B, D), V(Z + 1, B, D),
        V(*small, dtype=F32), V(2, T - 1, *small),
        sem(8),
        sem(Z), sem(Z), sem(Z), sem(Z, T), sem(Z, T), sem(Z, T), sem(Z, T), one, one,
        sem(3, Z), sem(3, Z), sem(3, Z, G), sem(3, Z, G), sem(3), sem(3), sem(3),
        sem(T, 4), sem(T, 4), sem(Z, U), sem(Z, U), sem(Z, U), sem(Z, T, U), sem(Z, T, U), one, one,
        sem(Z, T, 2), sem(Z, T, 2), sem(Z, 2), sem(Z + 1, 2),
        sem(2, T), sem(2, T),
    ]
    return pl.pallas_call(
        functools.partial(layer_kernel, n),
        out_shape=jax.ShapeDtypeStruct((B, D), F32),
        in_specs=[vmem] * 6 + [hbm] * 11,
        out_specs=vmem,
        scratch_shapes=scratch,
        compiler_params=pltpu.CompilerParams(
            collective_id=0, has_side_effects=True, vmem_limit_bytes=67043328
        ),
        name="layer",
    )(
        latent, rope_key.T, query_wide, query_narrow, trig, norm_gain.reshape(1, D),
        layer_input, key_up_wide, key_up_narrow, value_up_wide, value_up_narrow,
        out_wide, out_narrow, conv_weight, gate_weight, value_weight, down_weight,
    ).astype(BF)


def solution(mesh):
    in_specs = (
        P(("grp", "sp", "tp"), None),
        P(("grp", "sp"), None),
        P(("grp", "sp"), None),
        P(("grp", "sp"), "tp"),
        P(("grp", "sp"), "tp"),
        P(None, "tp"),
        P(None, "tp"),
        P(None, "tp"),
        P(None, "tp"),
        P("tp", None),
        P("tp", None),
        P(),
        P("sp", "tp"),
        P("sp", "tp"),
        P(None, "tp"),
        P("tp", "sp"),
    )
    out_specs = P(("grp", "sp", "tp"), None)
    return jax.shard_map(
        layer, mesh=mesh, in_specs=in_specs, out_specs=out_specs, check_vma=False
    )
```
